256 devices in a mesh: grp: 2 (over y), fs: 16 (over z), tp: 8 (over x, core).
Axes of the slice: x: 4, y: 2, z: 16, core: 2. Of those that a mesh axis runs over, the one named last changes fastest.
The devices are a block of a 4x16x16 slice.
Arguments:
- tokens: bfloat16 [32768, 2048], P(('grp', 'fs', 'tp')), parts along dimension 0, may hold values from -6 to 6
- route_ids: int32 [32768, 8], P(('grp', 'fs', 'tp')), parts along dimension 0, may hold values from 0 to 127, all different within a row; in each aligned block of 128 rows (0 to 127, 128 to 255, ...) at most 12 rows name the same one
- route_scores: float32 [32768, 8], P(('grp', 'fs', 'tp')), parts along dimension 0, may hold values from 0.05 to 1
- norm_gain: float32 [2048], P('fs'), may hold values from 0.1 to 1.9
- expert_gate: float32 [128, 2048, 256], P(None, 'fs', 'tp'), may hold values from -0.125 to 0.125
- expert_up: float32 [128, 2048, 256], P(None, 'fs', 'tp'), may hold values from -0.125 to 0.125
- expert_down: float32 [128, 256, 2048], P(None, 'fs', 'tp'), may hold values from -0.375 to 0.375
- shared_gate: float32 [2048, 256], P('fs', 'tp'), may hold values from -0.125 to 0.125
- shared_up: float32 [2048, 256], P('fs', 'tp'), may hold values from -0.125 to 0.125
- shared_down: float32 [256, 2048], P('fs', 'tp'), may hold values from -0.375 to 0.375
Outputs:
- mixed: bfloat16 [32768, 2048], P(('grp', 'fs', 'tp')), parts along dimension 0
- sampler_gate: bfloat16 [256, 2048, 256], P(('grp', 'fs', 'tp')), parts along dimension 0
- sampler_up: bfloat16 [256, 2048, 256], P(('grp', 'fs', 'tp')), parts along dimension 0
- sampler_down: bfloat16 [256, 256, 2048], P(('grp', 'fs', 'tp')), parts along dimension 0
- sampler_shared_gate: bfloat16 [4096, 256], P(('grp', 'fs')), parts along dimension 0
- sampler_shared_up: bfloat16 [4096, 256], P(('grp', 'fs')), parts along dimension 0
- sampler_shared_down: bfloat16 [512, 2048], P(('grp', 'fs')), parts along dimension 0
The draws below stay inside these ranges and needn't reach their ends.
There are 2 independent parts, one for each index of `grp`. The reference program is written for one: setup_inputs(seed, part) draws one part's arguments, and reference() takes and returns one part's arrays. A program takes and returns all parts, laid end to end along the dimension named above; an argument that names none is the same for every part. Nothing has to cross between parts.
Inputs may be any that keep to these rules, and one draw needn't show every extreme that they name: `route_ids`: each row names 8 different experts. Among the 128 rows of one device no expert is named more than 12 times, a bound that some block reaches.
All inputs are finite; a program needn't handle non-finite values.
Results may differ from the reference program's by a relative error of at most 0.0084.
Values may be sent and summed in bfloat16 or wider, within the bound.
A program may use at most 128 MiB of HBM per device.

```python
import math
import jax
import jax.numpy as jnp
import numpy as np
from jax import lax

D = 2048
F = 256
SH = 256
TOP_K = 8
TOK_DEV = 128
EXPERTS = 128
TOKENS = 16384
CAP = 12


def level_of(rng, extent, pieces, least, largest):
    def one(dim, blocks):
        draws = jax.random.uniform(jax.random.fold_in(jax.random.fold_in(rng, 6), dim), (blocks,), jnp.float32, least / len(pieces), largest / len(pieces))
        return jnp.repeat(jnp.exp(draws), extent[dim] // blocks).reshape((-1,) + (1,) * (len(extent) - dim - 1))

    factor_of = one(*pieces[0])
    for cut in pieces[1:]:
        factor_of = factor_of * one(*cut)
    return factor_of


def routed_block(own_key, own, number, rows, number_of, top, most, skew):
    ranking = jax.random.permutation(own_key, number_of)
    packed, usual = shares(number_of, rows * top, most, skew, True), shares(number_of, rows * top, most, skew, False)
    places = jnp.arange(number_of)

    def named(tallies, rotation):
        used = int((tallies > 0).sum())
        fixed = max(1, used // 4)
        moved = fixed + (places - fixed + rotation * (used - fixed)) % max(1, number_of - fixed)
        return jnp.zeros((number_of,), jnp.int32).at[ranking[jnp.where(places < fixed, places, moved)]].set(jnp.asarray(tallies, jnp.int32))

    tallies = jnp.where(number % 4 == 0, named(packed, number // 4), named(usual, number - number // 4 - 1))
    mixed = jax.random.permutation(jax.random.fold_in(own, 3), number_of)
    giver, taker = mixed[0:number_of // 2 * 2:2], mixed[1:number_of // 2 * 2:2]
    slack = jnp.minimum(tallies[giver] - 1, most - tallies[taker]) // 2
    slack = jnp.where((giver == ranking[0]) | (taker == ranking[0]) | (tallies[taker] == 0), 0, jnp.maximum(slack, 0))
    moved = jax.random.randint(jax.random.fold_in(own, 4), (number_of // 2,), 0, 1 << 20) % (slack + 1)
    tallies = tallies.at[giver].add(-moved).at[taker].add(moved)
    items = jnp.searchsorted(jnp.cumsum(tallies), jnp.arange(rows * top), side="right").astype(jnp.int32)
    listing = items.reshape(top, rows).T
    listing = listing[jax.random.permutation(jax.random.fold_in(own, 1), rows)]
    rotation = jax.random.randint(jax.random.fold_in(own, 2), (rows, 1), 0, top)
    return jnp.take_along_axis(listing, (jnp.arange(top)[None, :] + rotation) % top, axis=1)


def shares(amount, total, most, slope, full):
    weights = [(1 << 20) // math.isqrt(grade ** slope) + 1 for grade in range(1, amount + 1)]
    largest = most if full else min(most, max(-(-total // amount), total * weights[0] // sum(weights)))
    least = 1 if total - largest >= amount - 1 else 0
    given, surplus = [largest] + [least] * (amount - 1), total - largest - least * (amount - 1)
    while surplus > 0:
        movable = [i for i in range(1, amount) if given[i] < largest] or [i for i in range(1, amount) if given[i] < most]
        whole, left = sum([weights[i] for i in movable]), surplus
        for i in movable:
            addition = min(most - given[i], max(1, left * weights[i] // whole), surplus)
            given[i] = given[i] + addition
            surplus = surplus - addition
    return np.array(given)


def bell_draw(stream_key, shape, width, bound, pieces=(), held_as=jnp.bfloat16):
    result = jax.random.normal(stream_key, shape, jnp.float32) * width
    if len(pieces) > 0:
        result = level_of(stream_key, shape, pieces, -0.22, 0.18) * result
    return jnp.clip(result, min=-bound, max=bound).astype(held_as)


def setup_inputs(seed: int = 0, part: int = 0) -> dict:
    arg_keys = jax.random.split(jax.random.key(seed), 11)
    part_keys = jax.random.split(jax.random.fold_in(arg_keys[10], part), 11)
    tokens = bell_draw(part_keys[0], (TOKENS, D), 1.0, 6.0, ((0, 128),))
    route_ids_keys = jax.random.split(jax.random.fold_in(part_keys[1], 1), TOKENS // TOK_DEV)
    route_ids_turns = jax.random.permutation(jax.random.fold_in(part_keys[1], 3), TOKENS // TOK_DEV)
    route_ids = jax.vmap(lambda own, number: routed_block(jax.random.fold_in(part_keys[1], 2), own, number, TOK_DEV, EXPERTS, TOP_K, CAP, 1))(route_ids_keys, route_ids_turns).reshape((TOKENS, TOP_K))
    route_scores = jnp.clip(0.05 + 0.95 * jax.random.uniform(part_keys[2], (TOKENS, TOP_K), jnp.float32) ** level_of(part_keys[2], (TOKENS, TOP_K), ((0, 128),), -0.2, 0.2), 0.05, 1.0)
    norm_gain = jnp.clip(1.0 + 0.18 * jax.random.normal(arg_keys[3], (D,), jnp.float32), 0.1, 1.9)
    expert_gate = bell_draw(arg_keys[4], (EXPERTS, D, F), D ** -0.5, 0.125, ((1, 16), (2, 8)), jnp.float32)
    expert_up = bell_draw(arg_keys[5], (EXPERTS, D, F), D ** -0.5, 0.125, ((1, 16), (2, 8)), jnp.float32)
    expert_down = bell_draw(arg_keys[6], (EXPERTS, F, D), F ** -0.5, 0.375, ((1, 16), (2, 8)), jnp.float32)
    shared_gate = bell_draw(arg_keys[7], (D, SH), D ** -0.5, 0.125, ((0, 16), (1, 8)), jnp.float32)
    shared_up = bell_draw(arg_keys[8], (D, SH), D ** -0.5, 0.125, ((0, 16), (1, 8)), jnp.float32)
    shared_down = bell_draw(arg_keys[9], (SH, D), SH ** -0.5, 0.375, ((0, 16), (1, 8)), jnp.float32)
    return {"tokens": tokens, "route_ids": route_ids, "route_scores": route_scores, "norm_gain": norm_gain, "expert_gate": expert_gate, "expert_up": expert_up, "expert_down": expert_down, "shared_gate": shared_gate, "shared_up": shared_up, "shared_down": shared_down}


EPSILON = 1e-06
route_scale = 2.5

def reference(tokens, route_ids, route_scores, norm_gain, expert_gate, expert_up, expert_down, shared_gate, shared_up, shared_down):
    gain_col = norm_gain[:, None]
    sampler_gate = (gain_col[None] * expert_gate).astype(jnp.bfloat16)
    sampler_up = (gain_col[None] * expert_up).astype(jnp.bfloat16)
    sampler_down = expert_down.astype(jnp.bfloat16)
    sampler_shared_gate = (gain_col * shared_gate).astype(jnp.bfloat16)
    sampler_shared_up = (gain_col * shared_up).astype(jnp.bfloat16)
    sampler_shared_down = shared_down.astype(jnp.bfloat16)
    widened = tokens.astype(jnp.float32)
    normed = (widened * lax.rsqrt(lax.optimization_barrier(jnp.mean(widened * widened, axis=1, keepdims=True)) + EPSILON)).astype(jnp.bfloat16)
    weights = route_scale * route_scores / lax.optimization_barrier(jnp.sum(route_scores, axis=1, keepdims=True))
    gate_part = jnp.dot(normed, sampler_shared_gate, preferred_element_type=jnp.float32)
    up_part = jnp.dot(normed, sampler_shared_up, preferred_element_type=jnp.float32)
    shared_hidden = (jax.nn.silu(gate_part) * up_part).astype(jnp.bfloat16)
    shared_term = jnp.dot(shared_hidden, sampler_shared_down, preferred_element_type=jnp.float32)
    flat_ids = route_ids.reshape(-1)
    flat_weights = weights.reshape(-1)
    slots = EXPERTS * CAP

    def one_expert(expert, totals):
        matches = flat_ids == expert
        picked = jnp.nonzero(matches, size=slots, fill_value=0)[0].astype(jnp.int32)
        filled = (jnp.arange(slots, dtype=jnp.int32) < jnp.sum(matches.astype(jnp.int32))).astype(jnp.float32)
        owners = (picked // TOP_K).astype(jnp.int32)
        row_block = normed[owners]
        w_gate = lax.dynamic_index_in_dim(sampler_gate, expert, 0, keepdims=False)
        w_up = lax.dynamic_index_in_dim(sampler_up, expert, 0, keepdims=False)
        w_down = lax.dynamic_index_in_dim(sampler_down, expert, 0, keepdims=False)
        gate_rows = jnp.dot(row_block, w_gate, preferred_element_type=jnp.float32)
        up_rows = jnp.dot(row_block, w_up, preferred_element_type=jnp.float32)
        hidden = (jax.nn.silu(gate_rows) * up_rows).astype(jnp.bfloat16)
        produced = jnp.dot(hidden, w_down, preferred_element_type=jnp.float32).astype(jnp.bfloat16)
        factor = flat_weights[picked] * filled
        return totals.at[owners].add(produced.astype(jnp.float32) * factor[:, None])
    routed = lax.fori_loop(0, EXPERTS, one_expert, jnp.zeros(tokens.shape, jnp.float32))
    mixed = (routed + shared_term).astype(jnp.bfloat16)
    return (mixed, sampler_gate, sampler_up, sampler_down, sampler_shared_gate, sampler_shared_up, sampler_shared_down)
```

```python
import functools

import jax
import jax.numpy as jnp
import numpy as np
from jax import lax
from jax.experimental import pallas as pl
from jax.experimental.pallas import tpu as pltpu
from jax.sharding import PartitionSpec as P

EPSILON = 1e-06
route_scale = 2.5
ABSENT = -1024.0
MESH = pl.DeviceIdType.MESH
GROUP = 4
AG_PIECES = 2
RS_PIECES = 4
VMEM = pl.BlockSpec(memory_space=pltpu.VMEM)


def slot_of(offset):
    return 2 * offset if offset >= 0 else -2 * offset - 1


def greet(names_and_counts):
    barrier = pltpu.get_barrier_semaphore()
    total = 0
    for name, steps in names_and_counts:
        size = lax.axis_size(name)
        me = lax.axis_index(name)
        for step in steps:
            peer = lax.rem(me + step + size, size)
            pl.semaphore_signal(barrier, inc=1, device_id={name: peer}, device_id_type=MESH)
            total += 1
    return barrier, total


def remote(src, dst, send, recv, name, peer):
    return pltpu.make_async_remote_copy(
        src_ref=src, dst_ref=dst, send_sem=send, recv_sem=recv,
        device_id={name: peer}, device_id_type=MESH,
    )


def dispatch_kernel(
    n, m, cap, tok_ref, ids_ref, sc_ref, sgu_ref, sd_ref,
    x_ref, cw_ref, h_ref, hgu_ref, hd_ref,
    all_ref, meta_ref, stage_ref, pick_ref, gs_ref,
    ag_send, ag_recv, meta_send, meta_recv, x_send, x_recv, own_sem,
    gu_send, gu_recv, sd_send, sd_recv, gs_send, gs_recv,
):
    z, tp = lax.axis_index("fs"), lax.axis_index("tp")
    rows, width = tok_ref.shape
    picks = ids_ref.shape[0]
    up, down = lax.rem(z + 1, n), lax.rem(z + n - 1, n)
    wide = min(512, width)
    slots = GROUP * cap
    cols_f = sgu_ref.shape[1]
    own_h = gs_ref.shape[1]

    barrier, arrivals = greet((("fs", range(1, n)), ("tp", range(1, m))))
    widened = tok_ref[...].astype(jnp.float32)
    scale = lax.rsqrt(jnp.mean(widened * widened, axis=1, keepdims=True) + EPSILON)
    all_ref[pl.ds(0, rows), :] = (widened * scale).astype(jnp.bfloat16)
    scores = sc_ref[...]
    meta_ref[0, pl.ds(0, picks), :] = ids_ref[...].astype(jnp.float32)
    meta_ref[0, pl.ds(picks, picks), :] = route_scale * scores / jnp.sum(scores, axis=0, keepdims=True)
    hgu_ref[:, pl.ds(pl.multiple_of(tp * cols_f, cols_f), cols_f), :] = sgu_ref[...]
    hd_ref[:, pl.ds(pl.multiple_of(tp * sd_ref.shape[1], 128), sd_ref.shape[1])] = sd_ref[...]
    pl.semaphore_wait(barrier, arrivals)

    step_rows = rows // AG_PIECES

    def ring(k, p):
        src = max(k - 2, 0)
        peer = up if k % 2 == 1 else down
        return remote(
            all_ref.at[pl.ds(src * rows + p * step_rows, step_rows), :],
            all_ref.at[pl.ds(k * rows + p * step_rows, step_rows), :],
            ag_send.at[k, p], ag_recv.at[k, p], "fs", peer,
        )

    def ring_meta(k):
        peer = up if k % 2 == 1 else down
        return remote(meta_ref.at[max(k - 2, 0)], meta_ref.at[k], meta_send.at[k], meta_recv.at[k], "fs", peer)

    def gather_gu(q):
        return remote(
            sgu_ref,
            hgu_ref.at[:, pl.ds(pl.multiple_of(tp * cols_f, cols_f), cols_f), :],
            gu_send.at[q - 1], gu_recv.at[q - 1], "tp", lax.rem(tp + q, m),
        )

    def gather_sd(q):
        return remote(
            sd_ref,
            hd_ref.at[:, pl.ds(pl.multiple_of(tp * sd_ref.shape[1], 128), sd_ref.shape[1])],
            sd_send.at[q - 1], sd_recv.at[q - 1], "tp", lax.rem(tp + q, m),
        )

    def slice_gs(r):
        peer = lax.rem(z + r, n)
        return remote(
            hgu_ref.at[:, pl.ds(pl.multiple_of(peer * own_h, own_h), own_h), :],
            gs_ref.at[:, :, pl.ds(pl.multiple_of(z * 128, 128), 128)],
            gs_send.at[r - 1], gs_recv.at[r - 1], "fs", peer,
        )

    def exchange(g, q):
        peer = lax.rem(tp + q, m)
        return remote(stage_ref.at[g, peer], x_ref.at[g, tp], x_send.at[g, q - 1], x_recv.at[g, q - 1], "tp", peer)

    def own(g):
        return pltpu.make_async_copy(stage_ref.at[g, tp], x_ref.at[g, tp], own_sem.at[g])

    for k in (1, 2):
        ring_meta(k).start()
        for p in range(AG_PIECES):
            ring(k, p).start()
    for q in range(1, m):
        gather_gu(q).start()
        gather_sd(q).start()
    for q in range(1, m):
        gather_gu(q).wait_recv()
    for r in range(1, n):
        slice_gs(r).start()
    gs_ref[:, :, pl.ds(pl.multiple_of(z * 128, 128), 128)] = hgu_ref[
        :, pl.ds(pl.multiple_of(z * own_h, own_h), own_h), :
    ]

    before = lax.broadcasted_iota(jnp.int32, (rows, rows), 0) < lax.broadcasted_iota(jnp.int32, (rows, rows), 1)
    before = before.astype(jnp.float32).astype(jnp.bfloat16)
    served = (lax.broadcasted_iota(jnp.int32, (m, rows), 0) + m * z).astype(jnp.float32)
    places = lax.broadcasted_iota(jnp.int32, (slots, rows), 0).astype(jnp.float32)

    def select(g):
        for b in range(GROUP):
            k = g * GROUP + b
            meta = meta_ref[k]
            chosen = jnp.zeros((m, rows), jnp.float32)
            weight = jnp.zeros((m, rows), jnp.float32)
            for j in range(picks):
                hit = meta[j : j + 1, :] == served
                chosen = chosen + hit.astype(jnp.float32)
                weight = weight + jnp.where(hit, meta[picks + j : picks + j + 1, :], 0.0)
            rank = jnp.dot(chosen.astype(jnp.bfloat16), before, preferred_element_type=jnp.float32)
            code = jnp.where(chosen > 0.0, rank, ABSENT)
            cw_ref[k, pl.ds(0, m), :] = code
            cw_ref[k, pl.ds(m, m), :] = weight
            for q in range(m):
                hot = (jnp.broadcast_to(code[q : q + 1, :], (slots, rows)) + float(cap * b)) == places
                pick_ref[pl.ds(q * slots, slots), pl.ds(b * rows, rows)] = hot.astype(jnp.float32).astype(jnp.bfloat16)

        @pl.loop(0, width // wide)
        def _(c):
            cols = pl.ds(pl.multiple_of(c * wide, wide), wide)
            taken = jnp.dot(
                pick_ref[...], all_ref[pl.ds(g * GROUP * rows, GROUP * rows), cols],
                preferred_element_type=jnp.float32,
            ).astype(jnp.bfloat16)
            stage_ref[g, :, :, cols] = taken.reshape(m, slots, wide)

        for q in range(1, m):
            exchange(g, q).start()
        own(g).start()

    for k in range(1, n):
        ring_meta(k).wait_recv()
        if k + 2 < n:
            ring_meta(k + 2).start()
        for p in range(AG_PIECES):
            ring(k, p).wait_recv()
            if k + 2 < n:
                ring(k + 2, p).start()
        if k % GROUP == GROUP - 1:
            select(k // GROUP)

    for r in range(1, n):
        slice_gs(r).wait_recv()
    for g in range(n // GROUP):
        some = pl.ds(g * GROUP * rows, GROUP * rows)
        both = lax.dot_general(
            all_ref[some, :], gs_ref[...].reshape(2 * own_h, width), (((1,), (1,)), ((), ())),
            preferred_element_type=jnp.float32,
        )
        gate, upper = both[:, :own_h], both[:, own_h:]
        h_ref[some, :] = (gate / (1.0 + jnp.exp(-gate)) * upper).astype(jnp.bfloat16)

    for q in range(1, m):
        gather_gu(q).wait_send()
        gather_sd(q).wait()
    for r in range(1, n):
        slice_gs(r).wait_send()
    for k in range(1, n):
        ring_meta(k).wait_send()
        for p in range(AG_PIECES):
            ring(k, p).wait_send()
    for g in range(n // GROUP):
        own(g).wait()
        for q in range(1, m):
            exchange(g, q).wait()


def combine_kernel(
    n, m, cap, x_ref, gate_ref, up_ref, down_ref, cw_ref, h_ref, sd_ref, ecode_ref, ew_ref, place_ref,
    out_ref,
    y_ref, rv_ref, c_ref, d_ref, pin_ref, min_ref, pst_ref, mst_ref,
    y_send, y_recv, own_sem, p_send, p_recv, m_send, m_recv,
):
    z, tp = lax.axis_index("fs"), lax.axis_index("tp")
    rows, width = out_ref.shape
    upward, downward = lax.rem(z + 1, n), lax.rem(z + n - 1, n)
    wide = min(512, width)
    slots = GROUP * cap
    lanes = m * slots
    half = n // 2
    groups = n // GROUP
    part = rows // RS_PIECES

    barrier, arrivals = greet((("fs", (1, -1)), ("tp", range(1, m))))
    pl.semaphore_wait(barrier, arrivals)

    def exchange(g, q):
        peer = lax.rem(tp + q, m)
        return remote(y_ref.at[g, peer], rv_ref.at[g, tp], y_send.at[g, q - 1], y_recv.at[g, q - 1], "tp", peer)

    def own(g):
        return pltpu.make_async_copy(y_ref.at[g, tp], rv_ref.at[g, tp], own_sem.at[g])

    @pl.loop(0, groups)
    def _(i):
        g = groups - 1 - i
        x = x_ref[g]
        gate = jnp.dot(x, gate_ref[...], preferred_element_type=jnp.float32)
        upper = jnp.dot(x, up_ref[...], preferred_element_type=jnp.float32)
        hidden = (gate / (1.0 + jnp.exp(-gate)) * upper).astype(jnp.bfloat16)

        @pl.loop(0, width // wide)
        def _(c):
            cols = pl.ds(pl.multiple_of(c * wide, wide), wide)
            y = jnp.dot(hidden, down_ref[:, cols], preferred_element_type=jnp.float32)
            y_ref[g, :, :, cols] = y.astype(jnp.bfloat16).reshape(m, slots, wide)

        for q in range(1, m):
            exchange(g, q).start()
        own(g).start()

    def combine(g):
        own(g).wait()
        for q in range(1, m):
            exchange(g, q).wait_recv()
        some = pl.ds(g * GROUP * rows, GROUP * rows)
        exact = cw_ref[some, :]
        high = exact.astype(jnp.bfloat16)
        low = (exact - high.astype(jnp.float32)).astype(jnp.bfloat16)
        code = jnp.dot(high, ecode_ref[...], preferred_element_type=jnp.float32)
        high = jnp.dot(high, ew_ref[...], preferred_element_type=jnp.float32)
        low = jnp.dot(low, ew_ref[...], preferred_element_type=jnp.float32)
        for b in range(GROUP):
            span = slice(b * rows, (b + 1) * rows)
            hit = (code[span] + float(cap * b)) == place_ref[...]
            c_ref[pl.ds(b * rows, rows), pl.ds(0, lanes)] = jnp.where(hit, high[span], 0.0).astype(jnp.bfloat16)
            c_ref[pl.ds(b * rows, rows), pl.ds(lanes, lanes)] = jnp.where(hit, low[span], 0.0).astype(jnp.bfloat16)

        @pl.loop(0, width // wide)
        def _(c):
            cols = pl.ds(pl.multiple_of(c * wide, wide), wide)
            back = rv_ref[g, :, :, cols].reshape(lanes, wide)
            total = jnp.dot(c_ref[:, pl.ds(0, lanes)], back, preferred_element_type=jnp.float32)
            total += jnp.dot(c_ref[:, pl.ds(lanes, lanes)], back, preferred_element_type=jnp.float32)
            total += jnp.dot(h_ref[some, :], sd_ref[:, cols], preferred_element_type=jnp.float32)
            d_ref[g % 2, :, cols] = total

    def share(offset, c):
        k = slot_of(offset)
        return d_ref[(k // GROUP) % 2, pl.ds((k % GROUP) * rows + c * part, part), :]

    def hop(sign, r, c):
        some = pl.ds(c * part, part)
        if sign > 0:
            return remote(pst_ref.at[r - 1, some, :], pin_ref.at[r - 1, some, :],
                          p_send.at[r - 1, c], p_recv.at[r - 1, c], "fs", upward)
        return remote(mst_ref.at[r - 1, some, :], min_ref.at[r - 1, some, :],
                      m_send.at[r - 1, c], m_recv.at[r - 1, c], "fs", downward)

    def forward(sign, r, c):
        some = pl.ds(c * part, part)
        total = share(sign * r, c)
        if r < (half - 1 if sign > 0 else half):
            hop(sign, r + 1, c).wait_recv()
            total = total + (pin_ref if sign > 0 else min_ref)[r, some, :].astype(jnp.float32)
        (pst_ref if sign > 0 else mst_ref)[r - 1, some, :] = total.astype(jnp.bfloat16)
        hop(sign, r, c).start()

    combine(groups - 1)
    for i in range(half):
        for c in range(RS_PIECES):
            forward(-1, half - i, c)
            if half - 1 - i > 0:
                forward(1, half - 1 - i, c)
        if i % 2 == 0 and groups - 2 - i // 2 >= 0:
            combine(groups - 2 - i // 2)
    for c in range(RS_PIECES):
        some = pl.ds(c * part, part)
        hop(1, 1, c).wait_recv()
        hop(-1, 1, c).wait_recv()
        total = share(0, c) + pin_ref[0, some, :].astype(jnp.float32) + min_ref[0, some, :].astype(jnp.float32)
        out_ref[some, :] = total.astype(jnp.bfloat16)

    for c in range(RS_PIECES):
        for r in range(1, half):
            hop(1, r, c).wait_send()
        for r in range(1, half + 1):
            hop(-1, r, c).wait_send()
    for g in range(groups):
        for q in range(1, m):
            exchange(g, q).wait_send()


def on_device(
    tokens, route_ids, route_scores, norm_gain,
    expert_gate, expert_up, expert_down, shared_gate, shared_up, shared_down,
):
    n = lax.axis_size("fs")
    m = lax.axis_size("tp")
    experts = n * m
    rows, width = tokens.shape
    picks = route_ids.shape[1]
    cap = 3 * rows * picks // (2 * experts)
    slots = GROUP * cap
    groups = n // GROUP
    half = n // 2
    bf16, f32 = jnp.bfloat16, jnp.float32
    dma = pltpu.SemaphoreType.DMA

    deep, cols_f = expert_gate.shape[1:]
    down_rows, down_cols = expert_down.shape[1:]
    gate_t = (norm_gain[None, None, :] * jnp.swapaxes(expert_gate, 1, 2)).astype(bf16)
    up_t = (norm_gain[None, None, :] * jnp.swapaxes(expert_up, 1, 2)).astype(bf16)
    halves = down_cols // deep
    down_t = jnp.swapaxes(expert_down.astype(bf16).reshape(experts, down_rows, halves, deep), 1, 2)
    packed = jnp.concatenate([gate_t, up_t, down_t.reshape(experts, halves * down_rows, deep)], axis=1)
    moved = lax.all_to_all(packed, ("fs", "tp"), split_axis=0, concat_axis=0, tiled=True)
    moved = moved.reshape(n, m, packed.shape[1], deep)

    def served(tile):
        return jnp.transpose(tile, (0, 3, 1, 2)).reshape(n * deep, m * cols_f)

    served_gate = served(moved[:, :, :cols_f])
    served_up = served(moved[:, :, cols_f : 2 * cols_f])
    served_down = jnp.transpose(
        moved[:, :, 2 * cols_f :].reshape(n, m, halves, down_rows, deep), (0, 3, 1, 2, 4)
    ).reshape(n * down_rows, m * down_cols)

    shared_t = jnp.stack([
        (norm_gain[None, :] * shared_gate.T).astype(bf16), (norm_gain[None, :] * shared_up.T).astype(bf16),
    ])
    own_h = m * cols_f // n
    routed, codes, hidden, held_gu, held_down = pl.pallas_call(
        functools.partial(dispatch_kernel, n, m, cap),
        out_shape=(
            jax.ShapeDtypeStruct((groups, m, slots, width), bf16),
            jax.ShapeDtypeStruct((n, 2 * m, rows), f32),
            jax.ShapeDtypeStruct((n * rows, own_h), bf16),
            jax.ShapeDtypeStruct((2, m * cols_f, deep), bf16),
            jax.ShapeDtypeStruct((down_rows, m * down_cols), bf16),
        ),
        in_specs=[VMEM] * 5,
        out_specs=(VMEM,) * 5,
        scratch_shapes=[
            pltpu.VMEM((n * rows, width), bf16),
            pltpu.VMEM((n, 2 * picks, rows), f32),
            pltpu.VMEM((groups, m, slots, width), bf16),
            pltpu.VMEM((m * slots, GROUP * rows), bf16),
            pltpu.VMEM((2, own_h, width), bf16),
            dma((n, AG_PIECES)), dma((n, AG_PIECES)), dma((n,)), dma((n,)),
            dma((groups, m - 1)), dma((groups, m - 1)), dma((groups,)),
            dma((m - 1,)), dma((m - 1,)), dma((m - 1,)), dma((m - 1,)), dma((n - 1,)), dma((n - 1,)),
        ],
        compiler_params=pltpu.CompilerParams(
            collective_id=0, has_side_effects=True, vmem_limit_bytes=48 * 1024 * 1024,
        ),
        cost_estimate=pl.CostEstimate(flops=100_000_000_000, bytes_accessed=30_000_000, transcendentals=0),
        name="dispatch",
    )(tokens, route_ids.T, route_scores.T, shared_t, shared_down.astype(bf16))

    lane = np.arange(m * slots)
    expand = (lane[None, :] // slots == np.arange(2 * m)[:, None]).astype(np.float32)
    ecode = jnp.asarray(expand, bf16)
    ew = jnp.asarray(np.roll(expand, m, axis=0), bf16)
    place = jnp.asarray((lane % slots)[None, :].astype(np.float32))
    codes = jnp.transpose(codes, (0, 2, 1)).reshape(n * rows, 2 * m)
    mixed = pl.pallas_call(
        functools.partial(combine_kernel, n, m, cap),
        out_shape=jax.ShapeDtypeStruct((rows, width), bf16),
        in_specs=[VMEM] * 10,
        out_specs=VMEM,
        scratch_shapes=[
            pltpu.VMEM((groups, m, slots, width), bf16),
            pltpu.VMEM((groups, m, slots, width), bf16),
            pltpu.VMEM((GROUP * rows, 2 * m * slots), bf16),
            pltpu.VMEM((2, GROUP * rows, width), f32),
            pltpu.VMEM((half - 1, rows, width), bf16),
            pltpu.VMEM((half, rows, width), bf16),
            pltpu.VMEM((half - 1, rows, width), bf16),
            pltpu.VMEM((half, rows, width), bf16),
            dma((groups, m - 1)), dma((groups, m - 1)), dma((groups,)),
            dma((half - 1, RS_PIECES)), dma((half - 1, RS_PIECES)),
            dma((half, RS_PIECES)), dma((half, RS_PIECES)),
        ],
        compiler_params=pltpu.CompilerParams(
            collective_id=1, has_side_effects=True, vmem_limit_bytes=60 * 1024 * 1024,
        ),
        cost_estimate=pl.CostEstimate(flops=100_000_000_000, bytes_accessed=30_000_000, transcendentals=0),
        name="combine",
    )(
        routed.reshape(groups, m * slots, width), served_gate, served_up, served_down, codes, hidden, held_down,
        ecode, ew, place,
    )
    return (
        mixed, served_gate[None], served_up[None], served_down[None],
        held_gu[0].T, held_gu[1].T, held_down,
    )


def solution(mesh):
    return jax.shard_map(
        on_device,
        mesh=mesh,
        in_specs=(
            P(("grp", "fs", "tp"), None),
            P(("grp", "fs", "tp"), None),
            P(("grp", "fs", "tp"), None),
            P("fs"),
            P(None, "fs", "tp"),
            P(None, "fs", "tp"),
            P(None, "fs", "tp"),
            P("fs", "tp"),
            P("fs", "tp"),
            P("fs", "tp"),
        ),
        out_specs=(
            P(("grp", "fs", "tp"), None),
            P(("grp", "fs", "tp"), None, None),
            P(("grp", "fs", "tp"), None, None),
            P(("grp", "fs", "tp"), None, None),
            P(("grp", "fs"), None),
            P(("grp", "fs"), None),
            P(("grp", "fs"), None),
        ),
        check_vma=False,
    )
```

```python
import functools

import jax
import jax.numpy as jnp
import numpy as np
from jax import lax
from jax.experimental import pallas as pl
from jax.experimental.pallas import tpu as pltpu
from jax.sharding import PartitionSpec as P

EPSILON = 1e-06
route_scale = 2.5
ABSENT = -1024.0
MESH = pl.DeviceIdType.MESH
GROUP = 4
AG_PIECES = 2
W_FIRST, W_EVERY = 5, 4
VMEM = pl.BlockSpec(memory_space=pltpu.VMEM)


def slot_of(offset):
    return 2 * offset if offset >= 0 else -2 * offset - 1


def greet(names_and_counts):
    barrier = pltpu.get_barrier_semaphore()
    total = 0
    for name, steps in names_and_counts:
        size = lax.axis_size(name)
        me = lax.axis_index(name)
        for step in steps:
            peer = lax.rem(me + step + size, size)
            pl.semaphore_signal(barrier, inc=1, device_id={name: peer}, device_id_type=MESH)
            total += 1
    return barrier, total


def remote(src, dst, send, recv, name, peer):
    return pltpu.make_async_remote_copy(
        src_ref=src, dst_ref=dst, send_sem=send, recv_sem=recv,
        device_id={name: peer}, device_id_type=MESH,
    )


def offset_of(slot):
    return slot // 2 if slot % 2 == 0 else -((slot + 1) // 2)


def kernel(
    n, m, cap, tok_ref, ids_ref, sc_ref, sgu_ref, sd_ref, wg_ref, wu_ref, wd_ref, ecode_ref, ew_ref, place_ref,
    out_ref, gate_ref, up_ref, down_ref, hgu_ref, hd_ref,
    all_ref, meta_ref, cw_ref, stage_ref, x_ref, rv_ref, pick_ref, gs_ref, h_ref,
    mg_ref, mu_ref, md_ref, fg_ref, fu_ref, fd_ref, c_ref, d_ref, pin_ref, min_ref, pst_ref, mst_ref,
    ag_send, ag_recv, meta_send, meta_recv, x_send, x_recv, y_send, y_recv,
    gu_send, gu_recv, sd_send, sd_recv, gs_send, gs_recv,
    wz_send, wz_recv, wz_own, wx_send, wx_recv, p_send, p_recv, m_send, m_recv,
):
    z, tp = lax.axis_index("fs"), lax.axis_index("tp")
    rows, width = tok_ref.shape
    picks = ids_ref.shape[0]
    above, below = lax.rem(z + 1, n), lax.rem(z + n - 1, n)
    parts, wide = stage_ref.shape[1], stage_ref.shape[4]
    slots = GROUP * cap
    lanes = m * slots
    half, groups = n // 2, n // GROUP
    cols_f, deep = sgu_ref.shape[1:]
    own_h = gs_ref.shape[1]
    down_rows, down_cols = sd_ref.shape

    def tp_rows(size):
        return pl.ds(pl.multiple_of(tp * size, size), size)

    barrier, arrivals = greet((("fs", range(1, n)), ("tp", range(1, m))))
    widened = tok_ref[...].astype(jnp.float32)
    scale = lax.rsqrt(jnp.mean(widened * widened, axis=1, keepdims=True) + EPSILON)
    all_ref[pl.ds(0, rows), :] = (widened * scale).astype(jnp.bfloat16)
    scores = sc_ref[...]
    meta_ref[0, pl.ds(0, picks), :] = ids_ref[...].astype(jnp.float32)
    meta_ref[0, pl.ds(picks, picks), :] = route_scale * scores / jnp.sum(scores, axis=0, keepdims=True)
    hgu_ref[:, tp_rows(cols_f), :] = sgu_ref[...]
    hd_ref[:, tp_rows(down_cols)] = sd_ref[...]
    pl.semaphore_wait(barrier, arrivals)

    step_rows = rows // AG_PIECES

    def ring(k, p):
        src = max(k - 2, 0)
        return remote(
            all_ref.at[pl.ds(src * rows + p * step_rows, step_rows), :],
            all_ref.at[pl.ds(k * rows + p * step_rows, step_rows), :],
            ag_send.at[k, p], ag_recv.at[k, p], "fs", above if k % 2 == 1 else below,
        )

    def ring_meta(k):
        return remote(
            meta_ref.at[max(k - 2, 0)], meta_ref.at[k], meta_send.at[k], meta_recv.at[k],
            "fs", above if k % 2 == 1 else below,
        )

    def gather_gu(q):
        return remote(
            sgu_ref, hgu_ref.at[:, tp_rows(cols_f), :], gu_send.at[q - 1], gu_recv.at[q - 1], "tp", lax.rem(tp + q, m)
        )

    def gather_sd(q):
        return remote(
            sd_ref, hd_ref.at[:, tp_rows(down_cols)], sd_send.at[q - 1], sd_recv.at[q - 1], "tp", lax.rem(tp + q, m)
        )

    def slice_gs(r):
        peer = lax.rem(z + r, n)
        return remote(
            hgu_ref.at[:, pl.ds(pl.multiple_of(peer * own_h, own_h), own_h), :],
            gs_ref.at[:, :, pl.ds(pl.multiple_of(z * deep, deep), deep)],
            gs_send.at[r - 1], gs_recv.at[r - 1], "fs", peer,
        )

    kinds = (
        (wg_ref, mg_ref, fg_ref), (wu_ref, mu_ref, fu_ref), (wd_ref, md_ref, fd_ref),
    )

    def mid_place(kind, first, count):
        if kind < 2:
            return (slice(None), slice(None), pl.ds(first * deep, count * deep))
        return (slice(None), pl.ds(first * down_rows, count * down_rows), slice(None))

    def weight_z(w, s, kind):
        peer = lax.rem(z + n - offset_of(s), n)
        src, mid, _ = kinds[kind]
        return remote(
            src.at[peer], mid.at[mid_place(kind, s, 1)], wz_send.at[w, kind], wz_recv.at[w, kind], "fs", peer
        )

    def weight_own(kind):
        src, mid, _ = kinds[kind]
        return pltpu.make_async_copy(src.at[z], mid.at[mid_place(kind, 0, 1)], wz_own.at[kind])

    def weight_group(w):
        return range(max(1, w * GROUP), (w + 1) * GROUP)

    def weight_z_all(w, kind):
        of = weight_group(w)
        src, mid, _ = kinds[kind]
        return remote(
            src.at[pl.ds(0, len(of))], mid.at[mid_place(kind, of[0], len(of))],
            wz_send.at[w, kind], wz_recv.at[w, kind], "fs", above,
        )

    def piece(w, kind, who):
        if kind < 2:
            return who, slice(None), pl.ds(w * GROUP * deep, GROUP * deep)
        return who, pl.ds(w * GROUP * down_rows, GROUP * down_rows), slice(None)

    def landing(w, kind, where):
        if kind < 2:
            return where, pl.ds(w * GROUP * deep, GROUP * deep)
        return pl.ds(w * GROUP * down_rows, GROUP * down_rows), where

    def weight_x(w, q, kind):
        peer = lax.rem(tp + q, m)
        _, mid, final = kinds[kind]
        where = tp_rows(cols_f if kind < 2 else down_cols)
        return remote(
            mid.at[piece(w, kind, peer)], final.at[landing(w, kind, where)],
            wx_send.at[w, kind], wx_recv.at[w, kind], "tp", peer,
        )

    def weight_x_all(w, kind):
        _, mid, final = kinds[kind]
        where = pl.ds(0, (m - 1) * (cols_f if kind < 2 else down_cols))
        return remote(
            mid.at[piece(w, kind, pl.ds(0, m - 1))], final.at[landing(w, kind, where)],
            wx_send.at[w, kind], wx_recv.at[w, kind], "tp", lax.rem(tp + 1, m),
        )

    def exchange(g, q):
        peer = lax.rem(tp + q, m)
        return remote(stage_ref.at[g, :, peer], x_ref.at[g, :, tp], x_send.at[g], x_recv.at[g], "tp", peer)

    def exchange_all(g):
        some = pl.ds(0, m - 1)
        return remote(
            stage_ref.at[g, :, some], x_ref.at[g, :, some], x_send.at[g], x_recv.at[g], "tp", lax.rem(tp + 1, m)
        )

    def answer(g, c, q):
        peer = lax.rem(tp + q, m)
        return remote(stage_ref.at[g, c, peer], rv_ref.at[g, c, tp], y_send.at[g, c], y_recv.at[g, c], "tp", peer)

    def answer_all(g, c):
        some = pl.ds(0, m - 1)
        return remote(
            stage_ref.at[g, c, some], rv_ref.at[g, c, some], y_send.at[g, c], y_recv.at[g, c], "tp", lax.rem(tp + 1, m)
        )

    for k in (1, 2):
        ring_meta(k).start()
        for p in range(AG_PIECES):
            ring(k, p).start()
    for kind in range(3):
        weight_own(kind).start()
    for q in range(1, m):
        gather_gu(q).start()
        gather_sd(q).start()
    for q in range(1, m):
        gather_gu(q).wait_recv()
    for r in range(1, n):
        slice_gs(r).start()
    gs_ref[:, :, pl.ds(pl.multiple_of(z * deep, deep), deep)] = hgu_ref[
        :, pl.ds(pl.multiple_of(z * own_h, own_h), own_h), :
    ]

    before = lax.broadcasted_iota(jnp.int32, (rows, rows), 0) < lax.broadcasted_iota(jnp.int32, (rows, rows), 1)
    before = before.astype(jnp.float32).astype(jnp.bfloat16)
    served = (lax.broadcasted_iota(jnp.int32, (m, rows), 0) + m * z).astype(jnp.float32)
    places = lax.broadcasted_iota(jnp.int32, (slots, rows), 0).astype(jnp.float32)

    def select(g):
        for b in range(GROUP):
            k = g * GROUP + b
            meta = meta_ref[k]
            chosen = jnp.zeros((m, rows), jnp.float32)
            weight = jnp.zeros((m, rows), jnp.float32)
            for j in range(picks):
                hit = meta[j : j + 1, :] == served
                chosen = chosen + hit.astype(jnp.float32)
                weight = weight + jnp.where(hit, meta[picks + j : picks + j + 1, :], 0.0)
            rank = jnp.dot(chosen.astype(jnp.bfloat16), before, preferred_element_type=jnp.float32)
            code = jnp.where(chosen > 0.0, rank, ABSENT)
            cw_ref[k, pl.ds(0, m), :] = code
            cw_ref[k, pl.ds(m, m), :] = weight
            for q in range(m):
                hot = (jnp.broadcast_to(code[q : q + 1, :], (slots, rows)) + float(cap * b)) == places
                pick_ref[pl.ds(q * slots, slots), pl.ds(b * rows, rows)] = hot.astype(jnp.float32).astype(jnp.bfloat16)

        @pl.loop(0, parts)
        def _(c):
            cols = pl.ds(pl.multiple_of(c * wide, wide), wide)
            taken = jnp.dot(
                pick_ref[...], all_ref[pl.ds(g * GROUP * rows, GROUP * rows), cols],
                preferred_element_type=jnp.float32,
            ).astype(jnp.bfloat16)
            stage_ref[g, c] = taken.reshape(m, slots, wide)
            x_ref[g, c, tp] = stage_ref[g, c, tp]

        for q in range(1, m):
            exchange(g, q).start()

    issue = {}
    for i, w in enumerate(reversed(range(groups))):
        issue.setdefault(max(1, min(n - 3, W_FIRST + W_EVERY * i)), []).append(w)
    for k in range(1, n):
        ring_meta(k).wait_recv()
        if k + 2 < n:
            ring_meta(k + 2).start()
        for p in range(AG_PIECES):
            ring(k, p).wait_recv()
            if k + 2 < n:
                ring(k + 2, p).start()
        for w in issue.get(k, ()):
            for s in reversed(weight_group(w)):
                for kind in range(3):
                    weight_z(w, s, kind).start()
        if k % GROUP == GROUP - 1:
            select(k // GROUP)

    for r in range(1, n):
        slice_gs(r).wait_recv()
    for g in range(groups):
        some = pl.ds(g * GROUP * rows, GROUP * rows)
        both = lax.dot_general(
            all_ref[some, :], gs_ref[...].reshape(2 * own_h, width), (((1,), (1,)), ((), ())),
            preferred_element_type=jnp.float32,
        )
        gate, upper = both[:, :own_h], both[:, own_h:]
        h_ref[some, :] = (gate / (1.0 + jnp.exp(-gate)) * upper).astype(jnp.bfloat16)

    for kind in range(3):
        weight_own(kind).wait()
    for w in reversed(range(groups)):
        for kind in range(3):
            weight_z_all(w, kind).wait_recv()
        for q in range(1, m):
            for kind in range(3):
                weight_x(w, q, kind).start()
        for kind, (_, mid, final) in enumerate(kinds):
            where = tp_rows(cols_f if kind < 2 else down_cols)
            final[landing(w, kind, where)] = mid[piece(w, kind, tp)]
    for w in reversed(range(groups)):
        for kind in range(3):
            weight_x_all(w, kind).wait_recv()
        for s in range(w * GROUP, (w + 1) * GROUP):
            source = lax.rem(z + n + offset_of(s), n)
            at = pl.ds(pl.multiple_of(source * deep, deep), deep)
            gate_ref[:, at] = fg_ref[:, pl.ds(s * deep, deep)]
            up_ref[:, at] = fu_ref[:, pl.ds(s * deep, deep)]
            down_ref[pl.ds(pl.multiple_of(source * down_rows, down_rows), down_rows), :] = fd_ref[
                pl.ds(s * down_rows, down_rows), :
            ]

    for g in range(groups):
        exchange_all(g).wait_send()
        exchange_all(g).wait_recv()

    def experts(first, count):
        @pl.loop(0, count)
        def _(i):
            g = first - i
            gate = jnp.zeros((lanes, gate_ref.shape[0]), jnp.float32)
            upper = jnp.zeros((lanes, gate_ref.shape[0]), jnp.float32)
            for c in range(parts):
                x = x_ref[g, c].reshape(lanes, wide)
                cols = pl.ds(c * wide, wide)
                nt = (((1,), (1,)), ((), ()))
                gate += lax.dot_general(x, gate_ref[:, cols], nt, preferred_element_type=jnp.float32)
                upper += lax.dot_general(x, up_ref[:, cols], nt, preferred_element_type=jnp.float32)
            hidden = (gate / (1.0 + jnp.exp(-gate)) * upper).astype(jnp.bfloat16)

            @pl.loop(0, parts)
            def _(c):
                cols = pl.ds(pl.multiple_of(c * wide, wide), wide)
                y = jnp.dot(hidden, down_ref[:, cols], preferred_element_type=jnp.float32)
                stage_ref[g, c] = y.astype(jnp.bfloat16).reshape(m, slots, wide)
                rv_ref[g, c, tp] = stage_ref[g, c, tp]
                for q in range(1, m):
                    answer(g, c, q).start()

    def spread(g):
        exact = jnp.transpose(cw_ref[pl.ds(g * GROUP, GROUP)].reshape(GROUP * 2 * m, rows))
        high = exact.astype(jnp.bfloat16)
        low = (exact - high.astype(jnp.float32)).astype(jnp.bfloat16)
        for b in range(GROUP):
            code = jnp.dot(high, ecode_ref[b], preferred_element_type=jnp.float32)
            hit = (code + float(cap * b)) == place_ref[...]
            for i, term in enumerate((high, low)):
                value = jnp.dot(term, ew_ref[b], preferred_element_type=jnp.float32)
                c_ref[pl.ds(b * rows, rows), pl.ds(i * lanes, lanes)] = jnp.where(hit, value, 0.0).astype(jnp.bfloat16)

    def combine(g, c):
        answer_all(g, c).wait_recv()
        some = pl.ds(g * GROUP * rows, GROUP * rows)
        cols = pl.ds(pl.multiple_of(c * wide, wide), wide)
        back = rv_ref[g, c].reshape(lanes, wide)
        total = jnp.dot(c_ref[:, pl.ds(0, lanes)], back, preferred_element_type=jnp.float32)
        total += jnp.dot(c_ref[:, pl.ds(lanes, lanes)], back, preferred_element_type=jnp.float32)
        total += jnp.dot(h_ref[some, :], hd_ref[:, cols], preferred_element_type=jnp.float32)
        d_ref[c] = total

    def share(offset, c):
        return d_ref[c, pl.ds((slot_of(offset) % GROUP) * rows, rows), :]

    def hop(sign, r, c):
        if sign > 0:
            return remote(pst_ref.at[r % 2, c], pin_ref.at[r - 1, c],
                          p_send.at[r - 1, c], p_recv.at[r - 1, c], "fs", above)
        return remote(mst_ref.at[r % 2, c], min_ref.at[r - 1, c],
                      m_send.at[r - 1, c], m_recv.at[r - 1, c], "fs", below)

    def forward(sign, r, c):
        last = half - 1 if sign > 0 else half
        total = share(sign * r, c)
        if r < last:
            hop(sign, r + 1, c).wait_recv()
            total = total + (pin_ref if sign > 0 else min_ref)[r, c].astype(jnp.float32)
        if r + 2 <= last:
            hop(sign, r + 2, c).wait_send()
        (pst_ref if sign > 0 else mst_ref)[r % 2, c] = total.astype(jnp.bfloat16)
        hop(sign, r, c).start()

    for q in range(1, m):
        gather_sd(q).wait_recv()
    early = min(2, groups)
    experts(groups - 1, early)
    spread(groups - 1)
    for i in range(half):
        g = groups - 1 - i // 2

        if i % 2 == 1 and g > 0:
            spread(g - 1)

        @pl.loop(0, parts)
        def _(c):
            if i == 0:
                combine(g, c)
            forward(-1, half - i, c)
            if half - 1 - i > 0:
                forward(1, half - 1 - i, c)
            if i % 2 == 1 and g > 0:
                combine(g - 1, c)

        if i == 0 and groups > early:
            experts(groups - 1 - early, groups - early)

    @pl.loop(0, parts)
    def _(c):
        hop(1, 1, c).wait_recv()
        hop(-1, 1, c).wait_recv()
        total = share(0, c) + pin_ref[0, c].astype(jnp.float32) + min_ref[0, c].astype(jnp.float32)
        out_ref[:, pl.ds(pl.multiple_of(c * wide, wide), wide)] = total.astype(jnp.bfloat16)

    for c in range(parts):
        for r in range(1, min(2, half - 1) + 1):
            hop(1, r, c).wait_send()
        for r in range(1, min(2, half) + 1):
            hop(-1, r, c).wait_send()
        for g in range(groups):
            answer_all(g, c).wait_send()
    for q in range(1, m):
        gather_gu(q).wait_send()
        gather_sd(q).wait_send()
    for r in range(1, n):
        slice_gs(r).wait_send()
    for k in range(1, n):
        ring_meta(k).wait_send()
        for p in range(AG_PIECES):
            ring(k, p).wait_send()
    for w in range(groups):
        for kind in range(3):
            weight_z_all(w, kind).wait_send()
            weight_x_all(w, kind).wait_send()


def on_device(
    tokens, route_ids, route_scores, norm_gain,
    expert_gate, expert_up, expert_down, shared_gate, shared_up, shared_down,
):
    n = lax.axis_size("fs")
    m = lax.axis_size("tp")
    experts = n * m
    rows, width = tokens.shape
    picks = route_ids.shape[1]
    cap = 3 * rows * picks // (2 * experts)
    slots = GROUP * cap
    lanes = m * slots
    groups = n // GROUP
    half = n // 2
    bf16, f32 = jnp.bfloat16, jnp.float32
    dma = pltpu.SemaphoreType.DMA
    wide = min(512, width)
    parts = width // wide

    deep, cols_f = expert_gate.shape[1:]
    down_rows, down_cols = expert_down.shape[1:]
    hidden = m * cols_f
    own_h = hidden // n

    def turned(weight):
        return (norm_gain[None, None, :] * jnp.swapaxes(weight, 1, 2)).astype(bf16).reshape(n, m, cols_f, deep)

    shared_t = jnp.stack([
        (norm_gain[None, :] * shared_gate.T).astype(bf16), (norm_gain[None, :] * shared_up.T).astype(bf16),
    ])
    lane = np.arange(lanes)
    row = np.arange(GROUP * 2 * m)
    block = np.arange(GROUP)

    def expand(first):
        wanted = block[:, None, None] * 2 * m + first + (lane // slots)[None, None, :]
        return jnp.asarray((row[None, :, None] == wanted).astype(np.float32), bf16)

    place = jnp.asarray((lane % slots)[None, :].astype(np.float32))
    held = pl.BlockSpec(memory_space=pl.ANY)
    mixed, gate_t, up_t, served_down, held_gu, held_down = pl.pallas_call(
        functools.partial(kernel, n, m, cap),
        out_shape=(
            jax.ShapeDtypeStruct((rows, width), bf16),
            jax.ShapeDtypeStruct((hidden, width), bf16),
            jax.ShapeDtypeStruct((hidden, width), bf16),
            jax.ShapeDtypeStruct((hidden, width), bf16),
            jax.ShapeDtypeStruct((2, hidden, deep), bf16),
            jax.ShapeDtypeStruct((down_rows, width), bf16),
        ),
        in_specs=[VMEM] * 5 + [held] * 3 + [VMEM] * 3,
        out_specs=(VMEM,) * 6,
        scratch_shapes=[
            pltpu.VMEM((n * rows, width), bf16),
            pltpu.VMEM((n, 2 * picks, rows), f32),
            pltpu.VMEM((n, 2 * m, rows), f32),
            pltpu.VMEM((groups, parts, m, slots, wide), bf16),
            pltpu.VMEM((groups, parts, m, slots, wide), bf16),
            pltpu.VMEM((groups, parts, m, slots, wide), bf16),
            pltpu.VMEM((lanes, GROUP * rows), bf16),
            pltpu.VMEM((2, own_h, width), bf16),
            pltpu.VMEM((n * rows, own_h), bf16),
            pltpu.VMEM((m, cols_f, width), bf16),
            pltpu.VMEM((m, cols_f, width), bf16),
            pltpu.VMEM((m, n * down_rows, down_cols), bf16),
            pltpu.VMEM((hidden, width), bf16),
            pltpu.VMEM((hidden, width), bf16),
            pltpu.VMEM((hidden, width), bf16),
            pltpu.VMEM((GROUP * rows, 2 * lanes), bf16),
            pltpu.VMEM((parts, GROUP * rows, wide), f32),
            pltpu.VMEM((half - 1, parts, rows, wide), bf16),
            pltpu.VMEM((half, parts, rows, wide), bf16),
            pltpu.VMEM((2, parts, rows, wide), bf16),
            pltpu.VMEM((2, parts, rows, wide), bf16),
            dma((n, AG_PIECES)), dma((n, AG_PIECES)), dma((n,)), dma((n,)),
            dma((groups,)), dma((groups,)), dma((groups, parts)), dma((groups, parts)),
            dma((m - 1,)), dma((m - 1,)), dma((m - 1,)), dma((m - 1,)), dma((n - 1,)), dma((n - 1,)),
            dma((groups, 3)), dma((groups, 3)), dma((3,)), dma((groups, 3)), dma((groups, 3)),
            dma((half - 1, parts)), dma((half - 1, parts)), dma((half, parts)), dma((half, parts)),
        ],
        compiler_params=pltpu.CompilerParams(
            collective_id=0, has_side_effects=True, vmem_limit_bytes=63 * 1024 * 1024,
        ),
        cost_estimate=pl.CostEstimate(flops=100_000_000_000, bytes_accessed=30_000_000, transcendentals=0),
        name="hand_over",
    )(
        tokens, route_ids.T, route_scores.T, shared_t, shared_down.astype(bf16),
        turned(expert_gate), turned(expert_up), expert_down.astype(bf16).reshape(n, m, down_rows, down_cols),
        expand(0), expand(m), place,
    )
    return (mixed, gate_t.T[None], up_t.T[None], served_down[None], held_gu[0].T, held_gu[1].T, held_down)


def solution(mesh):
    return jax.shard_map(
        on_device,
        mesh=mesh,
        in_specs=(
            P(("grp", "fs", "tp"), None),
            P(("grp", "fs", "tp"), None),
            P(("grp", "fs", "tp"), None),
            P("fs"),
            P(None, "fs", "tp"),
            P(None, "fs", "tp"),
            P(None, "fs", "tp"),
            P("fs", "tp"),
            P("fs", "tp"),
            P("fs", "tp"),
        ),
        out_specs=(
            P(("grp", "fs", "tp"), None),
            P(("grp", "fs", "tp"), None, None),
            P(("grp", "fs", "tp"), None, None),
            P(("grp", "fs", "tp"), None, None),
            P(("grp", "fs"), None),
            P(("grp", "fs"), None),
            P(("grp", "fs"), None),
        ),
        check_vma=False,
    )
```

```python
import functools

import jax
import jax.numpy as jnp
import numpy as np
from jax import lax
from jax.experimental import pallas as pl
from jax.experimental.pallas import tpu as pltpu
from jax.sharding import PartitionSpec as P

EPSILON = 1e-06
route_scale = 2.5
ABSENT = -1024.0
MESH = pl.DeviceIdType.MESH
GROUP = 4
AG_PIECES = 2
LOADS = 4
VMEM = pl.BlockSpec(memory_space=pltpu.VMEM)


def slot_of(offset):
    return 2 * offset if offset >= 0 else -2 * offset - 1


def greet(names_and_counts):
    barrier = pltpu.get_barrier_semaphore()
    total = 0
    for name, steps in names_and_counts:
        size = lax.axis_size(name)
        me = lax.axis_index(name)
        for step in steps:
            peer = lax.rem(me + step + size, size)
            pl.semaphore_signal(barrier, inc=1, device_id={name: peer}, device_id_type=MESH)
            total += 1
    return barrier, total


def remote(src, dst, send, recv, name, peer):
    return pltpu.make_async_remote_copy(
        src_ref=src, dst_ref=dst, send_sem=send, recv_sem=recv,
        device_id={name: peer}, device_id_type=MESH,
    )


def offset_of(slot):
    return slot // 2 if slot % 2 == 0 else -((slot + 1) // 2)


def weight_order(n):
    order, far, near = [0, n - 1], n - 2, 1
    while near <= far:
        order.append(far)
        if near < far:
            order.append(near)
        far, near = far - 1, near + 1
    return order


def kernel(
    n, m, cap, tok_ref, ids_ref, sc_ref, gain_ref, sg_ref, su_ref, sd32_ref, eg_ref, eu_ref, ed_ref,
    ecode_ref, ew_ref, place_ref,
    out_ref, gate_ref, up_ref, down_ref, hgu_ref, hd_ref,
    all_ref, meta_ref, cw_ref, stage_ref, x_ref, rv_ref, pick_ref, gs_ref,
    sgu_ref, sd_ref, eg32_ref, eu32_ref, ed32_ref, wg_ref, wu_ref, wd_ref,
    mg_ref, mu_ref, md_ref, fg_ref, fu_ref, fd_ref, c_ref, d_ref, pin_ref, min_ref, pst_ref, mst_ref,
    ag_send, ag_recv, meta_send, meta_recv, x_send, x_recv, y_send, y_recv,
    gu_send, gu_recv, sd_send, sd_recv, gs_send, gs_recv,
    load_sem, wz_send, wz_recv, wx_send, wx_recv, p_send, p_recv, m_send, m_recv,
):
    z, tp = lax.axis_index("fs"), lax.axis_index("tp")
    rows, width = tok_ref.shape
    picks = ids_ref.shape[0]
    above, below = lax.rem(z + 1, n), lax.rem(z + n - 1, n)
    parts, wide = stage_ref.shape[1], stage_ref.shape[3]
    slots = GROUP * cap
    lanes = m * slots
    half, groups = n // 2, n // GROUP
    cols_f, deep = sgu_ref.shape[1:]
    order = weight_order(n)
    own_h = gs_ref.shape[1]
    down_rows, down_cols = sd_ref.shape

    def tp_rows(size):
        return pl.ds(pl.multiple_of(tp * size, size), size)

    barrier, arrivals = greet((("fs", range(1, n)), ("tp", range(1, m))))
    widened = tok_ref[...].astype(jnp.float32)
    scale = lax.rsqrt(jnp.mean(widened * widened, axis=1, keepdims=True) + EPSILON)
    all_ref[pl.ds(0, rows), :] = (widened * scale).astype(jnp.bfloat16)
    scores = sc_ref[...]
    meta_ref[0, pl.ds(0, picks), :] = ids_ref[...].astype(jnp.float32)
    meta_ref[0, pl.ds(picks, picks), :] = route_scale * scores / jnp.sum(scores, axis=0, keepdims=True)
    gain = gain_ref[...]
    sgu_ref[0] = (gain * sg_ref[...]).astype(jnp.bfloat16)
    sgu_ref[1] = (gain * su_ref[...]).astype(jnp.bfloat16)
    sd_ref[...] = sd32_ref[...].astype(jnp.bfloat16)
    hgu_ref[:, tp_rows(cols_f), :] = sgu_ref[...]
    hd_ref[:, tp_rows(down_cols)] = sd_ref[...]
    pl.semaphore_wait(barrier, arrivals)

    step_rows = rows // AG_PIECES

    def ring(k, p):
        src = max(k - 2, 0)
        return remote(
            all_ref.at[pl.ds(src * rows + p * step_rows, step_rows), :],
            all_ref.at[pl.ds(k * rows + p * step_rows, step_rows), :],
            ag_send.at[k, p], ag_recv.at[k, p], "fs", above if k % 2 == 1 else below,
        )

    def ring_meta(k):
        return remote(
            meta_ref.at[max(k - 2, 0)], meta_ref.at[k], meta_send.at[k], meta_recv.at[k],
            "fs", above if k % 2 == 1 else below,
        )

    def gather_gu(q):
        return remote(
            sgu_ref, hgu_ref.at[:, tp_rows(cols_f), :], gu_send.at[q - 1], gu_recv.at[q - 1], "tp", lax.rem(tp + q, m)
        )

    def gather_sd(q):
        return remote(
            sd_ref, hd_ref.at[:, tp_rows(down_cols)], sd_send.at[q - 1], sd_recv.at[q - 1], "tp", lax.rem(tp + q, m)
        )

    def slice_gs(r):
        peer = lax.rem(z + r, n)
        return remote(
            hgu_ref.at[:, pl.ds(pl.multiple_of(peer * own_h, own_h), own_h), :],
            gs_ref.at[:, :, pl.ds(pl.multiple_of(z * deep, deep), deep)],
            gs_send.at[r - 1], gs_recv.at[r - 1], "fs", peer,
        )

    kinds = (
        (wg_ref, mg_ref, fg_ref), (wu_ref, mu_ref, fu_ref), (wd_ref, md_ref, fd_ref),
    )

    def mid_place(kind, first, count):
        if kind < 2:
            return (slice(None), slice(None), pl.ds(first * deep, count * deep))
        return (slice(None), pl.ds(first * down_rows, count * down_rows), slice(None))

    def weight_z(at, kind):
        peer = lax.rem(z + n - offset_of(order[at]), n)
        src, mid, _ = kinds[kind]
        w = at // GROUP
        return remote(
            src.at[peer], mid.at[mid_place(kind, at, 1)], wz_send.at[w, kind], wz_recv.at[w, kind], "fs", peer
        )

    def weight_z_all(w, kind):
        first = max(1, w * GROUP)
        count = (w + 1) * GROUP - first
        _, mid, _ = kinds[kind]
        return remote(
            mid.at[mid_place(kind, first, count)], mid.at[mid_place(kind, first, count)],
            wz_send.at[w, kind], wz_recv.at[w, kind], "fs", above,
        )

    def piece(w, kind, who):
        if kind < 2:
            return who, slice(None), pl.ds(w * GROUP * deep, GROUP * deep)
        return who, pl.ds(w * GROUP * down_rows, GROUP * down_rows), slice(None)

    def landing(w, kind, where):
        if kind < 2:
            return where, pl.ds(w * GROUP * deep, GROUP * deep)
        return pl.ds(w * GROUP * down_rows, GROUP * down_rows), where

    def weight_x(w, q, kind):
        peer = lax.rem(tp + q, m)
        _, mid, final = kinds[kind]
        where = tp_rows(cols_f if kind < 2 else down_cols)
        return remote(
            mid.at[piece(w, kind, peer)], final.at[landing(w, kind, where)],
            wx_send.at[w, kind], wx_recv.at[w, kind], "tp", peer,
        )

    def weight_x_all(w, kind):
        _, _, final = kinds[kind]
        where = pl.ds(0, (m - 1) * (cols_f if kind < 2 else down_cols))
        return remote(
            final.at[landing(w, kind, where)], final.at[landing(w, kind, where)],
            wx_send.at[w, kind], wx_recv.at[w, kind], "tp", lax.rem(tp + 1, m),
        )

    def of(who):
        return pl.ds(pl.multiple_of(who * slots, slots), slots)

    most = pl.ds(0, (m - 1) * slots)

    def exchange(g, q):
        peer = lax.rem(tp + q, m)
        return remote(stage_ref.at[g, :, of(peer)], x_ref.at[g, :, of(tp)], x_send.at[g], x_recv.at[g], "tp", peer)

    def exchange_all(g):
        return remote(
            stage_ref.at[g, :, most], x_ref.at[g, :, most], x_send.at[g], x_recv.at[g], "tp", lax.rem(tp + 1, m)
        )

    def answer(g, c, q):
        peer = lax.rem(tp + q, m)
        return remote(
            stage_ref.at[g, c, of(peer)], rv_ref.at[g, c, of(tp)], y_send.at[g, c], y_recv.at[g, c], "tp", peer
        )

    def answer_all(g, c):
        return remote(
            stage_ref.at[g, c, most], rv_ref.at[g, c, most], y_send.at[g, c], y_recv.at[g, c], "tp", lax.rem(tp + 1, m)
        )

    span = n // LOADS
    loads = ((eg_ref, eg32_ref), (eu_ref, eu32_ref), (ed_ref, ed32_ref))

    def load(i, kind):
        src, dst = loads[kind]
        return pltpu.make_async_copy(src.at[pl.ds(i * span, span)], dst.at[i % 2], load_sem.at[i % 2, kind])

    for kind in range(3):
        load(0, kind).start()
    for k in (1, 2):
        ring_meta(k).start()
        for p in range(AG_PIECES):
            ring(k, p).start()
    for q in range(1, m):
        gather_gu(q).start()
        gather_sd(q).start()
    for i in range(LOADS):
        for kind in range(3):
            if i + 1 < LOADS:
                load(i + 1, kind).start()
            load(i, kind).wait()
        some = pl.ds(i * span, span)
        wg_ref[some] = (gain * eg32_ref[i % 2]).astype(jnp.bfloat16)
        wu_ref[some] = (gain * eu32_ref[i % 2]).astype(jnp.bfloat16)
        wd_ref[some] = ed32_ref[i % 2].astype(jnp.bfloat16)
    for kind, (src, mid, _) in enumerate(kinds):
        mid[mid_place(kind, 0, 1)] = src[z]
    for q in range(1, m):
        gather_gu(q).wait_recv()
    for r in range(1, n):
        slice_gs(r).start()
    gs_ref[:, :, pl.ds(pl.multiple_of(z * deep, deep), deep)] = hgu_ref[
        :, pl.ds(pl.multiple_of(z * own_h, own_h), own_h), :
    ]

    before = lax.broadcasted_iota(jnp.int32, (rows, rows), 0) < lax.broadcasted_iota(jnp.int32, (rows, rows), 1)
    before = before.astype(jnp.float32).astype(jnp.bfloat16)
    served = (lax.broadcasted_iota(jnp.int32, (m, rows), 0) + m * z).astype(jnp.float32)
    places = lax.broadcasted_iota(jnp.int32, (slots, rows), 0).astype(jnp.float32)

    def select(g):
        for b in range(GROUP):
            k = g * GROUP + b
            meta = meta_ref[k]
            chosen = jnp.zeros((m, rows), jnp.float32)
            weight = jnp.zeros((m, rows), jnp.float32)
            for j in range(picks):
                hit = meta[j : j + 1, :] == served
                chosen = chosen + hit.astype(jnp.float32)
                weight = weight + jnp.where(hit, meta[picks + j : picks + j + 1, :], 0.0)
            rank = jnp.dot(chosen.astype(jnp.bfloat16), before, preferred_element_type=jnp.float32)
            code = jnp.where(chosen > 0.0, rank, ABSENT)
            cw_ref[k, pl.ds(0, m), :] = code
            cw_ref[k, pl.ds(m, m), :] = weight
            for q in range(m):
                hot = (jnp.broadcast_to(code[q : q + 1, :], (slots, rows)) + float(cap * b)) == places
                pick_ref[pl.ds(q * slots, slots), pl.ds(b * rows, rows)] = hot.astype(jnp.float32).astype(jnp.bfloat16)

        @pl.loop(0, parts)
        def _(c):
            cols = pl.ds(pl.multiple_of(c * wide, wide), wide)
            taken = jnp.dot(
                pick_ref[...], all_ref[pl.ds(g * GROUP * rows, GROUP * rows), cols],
                preferred_element_type=jnp.float32,
            ).astype(jnp.bfloat16)
            stage_ref[g, c] = taken
            x_ref[g, c, of(tp), :] = stage_ref[g, c, of(tp), :]

        for q in range(1, m):
            exchange(g, q).start()

    moved_on = []

    def move_on(w):
        moved_on.append(w)
        for kind in range(3):
            weight_z_all(w, kind).wait_recv()
        for q in range(1, m):
            for kind in range(3):
                weight_x(w, q, kind).start()
        for kind, (_, mid, final) in enumerate(kinds):
            where = tp_rows(cols_f if kind < 2 else down_cols)
            final[landing(w, kind, where)] = mid[piece(w, kind, tp)]

    issue = {}
    for at in range(1, n):
        issue.setdefault(max(1, min(n - 3, 1 + 2 * (at // 2))), []).append(at)
    for k in range(1, n):
        ring_meta(k).wait_recv()
        if k + 2 < n:
            ring_meta(k + 2).start()
        for p in range(AG_PIECES):
            ring(k, p).wait_recv()
            if k + 2 < n:
                ring(k + 2, p).start()
        for at in issue.get(k, ()):
            for kind in range(3):
                weight_z(at, kind).start()
        if k % GROUP == GROUP - 1:
            select(k // GROUP)
            if groups > 2 and k // GROUP >= groups - 2:
                move_on(k // GROUP - groups + 2)

    for r in range(1, n):
        slice_gs(r).wait_recv()
    for g in range(groups):
        some = pl.ds(g * GROUP * rows, GROUP * rows)
        both = lax.dot_general(
            all_ref[some, :], gs_ref[...].reshape(2 * own_h, width), (((1,), (1,)), ((), ())),
            preferred_element_type=jnp.float32,
        )
        gate, upper = both[:, :own_h], both[:, own_h:]
        c_ref[g, :, pl.ds(lanes, own_h)] = (gate / (1.0 + jnp.exp(-gate)) * upper).astype(jnp.bfloat16)
        turned = jnp.transpose(cw_ref[pl.ds(g * GROUP, GROUP)].reshape(GROUP * 2 * m, rows)).astype(jnp.bfloat16)
        for b in range(GROUP):
            code = jnp.dot(turned, ecode_ref[b], preferred_element_type=jnp.float32)
            value = jnp.dot(turned, ew_ref[b], preferred_element_type=jnp.float32)
            hit = (code + float(cap * b)) == place_ref[...]
            c_ref[g, pl.ds(b * rows, rows), pl.ds(0, lanes)] = jnp.where(hit, value, 0.0).astype(jnp.bfloat16)
    for q in range(1, m):
        gather_sd(q).wait_recv()
    for g in range(groups):
        for c in range(parts):
            rv_ref[g, c, pl.ds(lanes, own_h), :] = hd_ref[:, pl.ds(c * wide, wide)]

    for w in range(groups):
        if w not in moved_on:
            move_on(w)
    for w in range(groups):
        for kind in range(3):
            weight_x_all(w, kind).wait_recv()
        for at in range(w * GROUP, (w + 1) * GROUP):
            source = lax.rem(z + n + offset_of(order[at]), n)
            there = pl.ds(pl.multiple_of(source * deep, deep), deep)
            gate_ref[:, there] = fg_ref[:, pl.ds(at * deep, deep)]
            up_ref[:, there] = fu_ref[:, pl.ds(at * deep, deep)]
            down_ref[pl.ds(pl.multiple_of(source * down_rows, down_rows), down_rows), :] = fd_ref[
                pl.ds(at * down_rows, down_rows), :
            ]

    for g in range(groups):
        exchange_all(g).wait_send()
        exchange_all(g).wait_recv()

    def experts(first, count):
        @pl.loop(0, count)
        def _(i):
            g = first - i
            gate = jnp.zeros((lanes, gate_ref.shape[0]), jnp.float32)
            upper = jnp.zeros((lanes, gate_ref.shape[0]), jnp.float32)
            for c in range(parts):
                x = x_ref[g, c]
                cols = pl.ds(c * wide, wide)
                nt = (((1,), (1,)), ((), ()))
                gate += lax.dot_general(x, gate_ref[:, cols], nt, preferred_element_type=jnp.float32)
                upper += lax.dot_general(x, up_ref[:, cols], nt, preferred_element_type=jnp.float32)
            hidden = (gate / (1.0 + jnp.exp(-gate)) * upper).astype(jnp.bfloat16)

            @pl.loop(0, parts)
            def _(c):
                cols = pl.ds(pl.multiple_of(c * wide, wide), wide)
                y = jnp.dot(hidden, down_ref[:, cols], preferred_element_type=jnp.float32)
                stage_ref[g, c] = y.astype(jnp.bfloat16)
                rv_ref[g, c, of(tp), :] = stage_ref[g, c, of(tp), :]
                for q in range(1, m):
                    answer(g, c, q).start()

    def combine(g, c):
        answer_all(g, c).wait_recv()
        d_ref[c] = jnp.dot(c_ref[g], rv_ref[g, c], preferred_element_type=jnp.float32)

    def share(offset, c):
        return d_ref[c, pl.ds((slot_of(offset) % GROUP) * rows, rows), :]

    def hop(sign, r, c):
        if sign > 0:
            return remote(pst_ref.at[r % 2, c], pin_ref.at[r - 1, c],
                          p_send.at[r - 1, c], p_recv.at[r - 1, c], "fs", above)
        return remote(mst_ref.at[r % 2, c], min_ref.at[r - 1, c],
                      m_send.at[r - 1, c], m_recv.at[r - 1, c], "fs", below)

    def forward(sign, r, c):
        last = half - 1 if sign > 0 else half
        total = share(sign * r, c)
        if r < last:
            hop(sign, r + 1, c).wait_recv()
            total = total + (pin_ref if sign > 0 else min_ref)[r, c].astype(jnp.float32)
        if r + 2 <= last:
            hop(sign, r + 2, c).wait_send()
        (pst_ref if sign > 0 else mst_ref)[r % 2, c] = total.astype(jnp.bfloat16)
        hop(sign, r, c).start()

    early = min(2, groups)
    experts(groups - 1, early)
    for i in range(half):
        g = groups - 1 - i // 2

        @pl.loop(0, parts)
        def _(c):
            if i == 0:
                combine(g, c)
            forward(-1, half - i, c)
            if half - 1 - i > 0:
                forward(1, half - 1 - i, c)
            if i % 2 == 1 and g > 0:
                combine(g - 1, c)

        if i == 0 and groups > early:
            experts(groups - 1 - early, groups - early)

    @pl.loop(0, parts)
    def _(c):
        hop(1, 1, c).wait_recv()
        hop(-1, 1, c).wait_recv()
        total = share(0, c) + pin_ref[0, c].astype(jnp.float32) + min_ref[0, c].astype(jnp.float32)
        out_ref[:, pl.ds(pl.multiple_of(c * wide, wide), wide)] = total.astype(jnp.bfloat16)

    for c in range(parts):
        for r in range(1, min(2, half - 1) + 1):
            hop(1, r, c).wait_send()
        for r in range(1, min(2, half) + 1):
            hop(-1, r, c).wait_send()
        for g in range(groups):
            answer_all(g, c).wait_send()
    for q in range(1, m):
        gather_gu(q).wait_send()
        gather_sd(q).wait_send()
    for r in range(1, n):
        slice_gs(r).wait_send()
    for k in range(1, n):
        ring_meta(k).wait_send()
        for p in range(AG_PIECES):
            ring(k, p).wait_send()
    for w in range(groups):
        for kind in range(3):
            weight_z_all(w, kind).wait_send()
            weight_x_all(w, kind).wait_send()


def on_device(
    tokens, route_ids, route_scores, norm_gain,
    expert_gate, expert_up, expert_down, shared_gate, shared_up, shared_down,
):
    n = lax.axis_size("fs")
    m = lax.axis_size("tp")
    experts = n * m
    rows, width = tokens.shape
    picks = route_ids.shape[1]
    cap = 3 * rows * picks // (2 * experts)
    slots = GROUP * cap
    lanes = m * slots
    groups = n // GROUP
    half = n // 2
    bf16, f32 = jnp.bfloat16, jnp.float32
    dma = pltpu.SemaphoreType.DMA
    wide = min(512, width)
    parts = width // wide

    deep, cols_f = expert_gate.shape[1:]
    down_rows, down_cols = expert_down.shape[1:]
    hidden = m * cols_f
    own_h = hidden // n

    def turned(weight):
        return jnp.swapaxes(weight, 1, 2).reshape(n, m, cols_f, deep)

    lane = np.arange(lanes)
    row = np.arange(GROUP * 2 * m)
    block = np.arange(GROUP)

    def expand(first):
        wanted = block[:, None, None] * 2 * m + first + (lane // slots)[None, None, :]
        return jnp.asarray((row[None, :, None] == wanted).astype(np.float32), bf16)

    place = jnp.asarray((lane % slots)[None, :].astype(np.float32))
    held = pl.BlockSpec(memory_space=pl.ANY)
    mixed, gate_t, up_t, served_down, held_gu, held_down = pl.pallas_call(
        functools.partial(kernel, n, m, cap),
        out_shape=(
            jax.ShapeDtypeStruct((rows, width), bf16),
            jax.ShapeDtypeStruct((hidden, width), bf16),
            jax.ShapeDtypeStruct((hidden, width), bf16),
            jax.ShapeDtypeStruct((hidden, width), bf16),
            jax.ShapeDtypeStruct((2, hidden, deep), bf16),
            jax.ShapeDtypeStruct((down_rows, width), bf16),
        ),
        in_specs=[VMEM] * 7 + [held] * 3 + [VMEM] * 3,
        out_specs=(VMEM,) * 6,
        scratch_shapes=[
            pltpu.VMEM((n * rows, width), bf16),
            pltpu.VMEM((n, 2 * picks, rows), f32),
            pltpu.VMEM((n, 2 * m, rows), f32),
            pltpu.VMEM((groups, parts, lanes, wide), bf16),
            pltpu.VMEM((groups, parts, lanes, wide), bf16),
            pltpu.VMEM((groups, parts, lanes + own_h, wide), bf16),
            pltpu.VMEM((lanes, GROUP * rows), bf16),
            pltpu.VMEM((2, own_h, width), bf16),
            pltpu.VMEM((2, cols_f, deep), bf16),
            pltpu.VMEM((down_rows, down_cols), bf16),
            pltpu.VMEM((2, n // LOADS, m, cols_f, deep), f32),
            pltpu.VMEM((2, n // LOADS, m, cols_f, deep), f32),
            pltpu.VMEM((2, n // LOADS, m, down_rows, down_cols), f32),
            pltpu.VMEM((n, m, cols_f, deep), bf16),
            pltpu.VMEM((n, m, cols_f, deep), bf16),
            pltpu.VMEM((n, m, down_rows, down_cols), bf16),
            pltpu.VMEM((m, cols_f, width), bf16),
            pltpu.VMEM((m, cols_f, width), bf16),
            pltpu.VMEM((m, n * down_rows, down_cols), bf16),
            pltpu.VMEM((hidden, width), bf16),
            pltpu.VMEM((hidden, width), bf16),
            pltpu.VMEM((hidden, width), bf16),
            pltpu.VMEM((groups, GROUP * rows, lanes + own_h), bf16),
            pltpu.VMEM((parts, GROUP * rows, wide), f32),
            pltpu.VMEM((half - 1, parts, rows, wide), bf16),
            pltpu.VMEM((half, parts, rows, wide), bf16),
            pltpu.VMEM((2, parts, rows, wide), bf16),
            pltpu.VMEM((2, parts, rows, wide), bf16),
            dma((n, AG_PIECES)), dma((n, AG_PIECES)), dma((n,)), dma((n,)),
            dma((groups,)), dma((groups,)), dma((groups, parts)), dma((groups, parts)),
            dma((m - 1,)), dma((m - 1,)), dma((m - 1,)), dma((m - 1,)), dma((n - 1,)), dma((n - 1,)),
            dma((2, 3)), dma((groups, 3)), dma((groups, 3)), dma((groups, 3)), dma((groups, 3)),
            dma((half - 1, parts)), dma((half - 1, parts)), dma((half, parts)), dma((half, parts)),
        ],
        compiler_params=pltpu.CompilerParams(
            collective_id=0, has_side_effects=True, vmem_limit_bytes=63 * 1024 * 1024,
        ),
        cost_estimate=pl.CostEstimate(flops=100_000_000_000, bytes_accessed=30_000_000, transcendentals=0),
        name="hand_over",
    )(
        tokens, route_ids.T, route_scores.T, norm_gain[None, :], shared_gate.T, shared_up.T, shared_down,
        turned(expert_gate), turned(expert_up), expert_down.reshape(n, m, down_rows, down_cols),
        expand(0), expand(m), place,
    )
    return (mixed, gate_t.T[None], up_t.T[None], served_down[None], held_gu[0].T, held_gu[1].T, held_down)


def solution(mesh):
    return jax.shard_map(
        on_device,
        mesh=mesh,
        in_specs=(
            P(("grp", "fs", "tp"), None),
            P(("grp", "fs", "tp"), None),
            P(("grp", "fs", "tp"), None),
            P("fs"),
            P(None, "fs", "tp"),
            P(None, "fs", "tp"),
            P(None, "fs", "tp"),
            P("fs", "tp"),
            P("fs", "tp"),
            P("fs", "tp"),
        ),
        out_specs=(
            P(("grp", "fs", "tp"), None),
            P(("grp", "fs", "tp"), None, None),
            P(("grp", "fs", "tp"), None, None),
            P(("grp", "fs", "tp"), None, None),
            P(("grp", "fs"), None),
            P(("grp", "fs"), None),
            P(("grp", "fs"), None),
        ),
        check_vma=False,
    )
```

```python
import functools

import jax
import jax.numpy as jnp
import numpy as np
from jax import lax
from jax.experimental import pallas as pl
from jax.experimental.pallas import tpu as pltpu
from jax.sharding import PartitionSpec as P

EPSILON = 1e-06
route_scale = 2.5
ABSENT = -1024.0
MESH = pl.DeviceIdType.MESH
GROUP = 4
AG_PIECES = 2
LOADS = 4
VMEM = pl.BlockSpec(memory_space=pltpu.VMEM)


def slot_of(offset):
    return 2 * offset if offset >= 0 else -2 * offset - 1


def greet(names_and_counts):
    barrier = pltpu.get_barrier_semaphore()
    total = 0
    for name, steps in names_and_counts:
        size = lax.axis_size(name)
        me = lax.axis_index(name)
        for step in steps:
            peer = lax.rem(me + step + size, size)
            pl.semaphore_signal(barrier, inc=1, device_id={name: peer}, device_id_type=MESH)
            total += 1
    return barrier, total


def remote(src, dst, send, recv, name, peer):
    return pltpu.make_async_remote_copy(
        src_ref=src, dst_ref=dst, send_sem=send, recv_sem=recv,
        device_id={name: peer}, device_id_type=MESH,
    )


def offset_of(slot):
    return slot // 2 if slot % 2 == 0 else -((slot + 1) // 2)


def weight_order(n):
    order, far, near = [0, n - 1], n - 2, 1
    while near <= far:
        order.append(far)
        if near < far:
            order.append(near)
        far, near = far - 1, near + 1
    return order


def kernel(
    n, m, cap, tok_ref, ids_ref, sc_ref, gain_ref, sg_ref, su_ref, sd32_ref, eg_ref, eu_ref, ed_ref,
    ecode_ref, ew_ref, place_ref,
    out_ref, gate_ref, up_ref, down_ref, hgu_ref, hd_ref,
    all_ref, meta_ref, cw_ref, stage_ref, x_ref, rv_ref, pick_ref, gs_ref,
    sgu_ref, sd_ref, eg32_ref, eu32_ref, ed32_ref, wg_ref, wu_ref, wd_ref,
    mg_ref, mu_ref, md_ref, fg_ref, fu_ref, fd_ref, c_ref, d_ref, pin_ref, min_ref, pst_ref, mst_ref,
    ag_send, ag_recv, meta_send, meta_recv, x_send, x_recv, y_send, y_recv,
    gu_send, gu_recv, sd_send, sd_recv, gs_send, gs_recv,
    load_sem, wz_send, wz_recv, wx_send, wx_recv, p_send, p_recv, m_send, m_recv,
):
    z, tp = lax.axis_index("fs"), lax.axis_index("tp")
    rows, width = tok_ref.shape
    picks = ids_ref.shape[0]
    above, below = lax.rem(z + 1, n), lax.rem(z + n - 1, n)
    parts, wide = stage_ref.shape[1], stage_ref.shape[3]
    slots = GROUP * cap
    lanes = m * slots
    half, groups = n // 2, n // GROUP
    cols_f, deep = sgu_ref.shape[1:]
    order = weight_order(n)
    bundles = [(first, GROUP) for first in range(0, n - GROUP, GROUP)] + [(n - GROUP, GROUP - 1), (n - 1, 1)]
    bundle_of = [w for w, (_, count) in enumerate(bundles) for _ in range(count)]
    own_h = gs_ref.shape[1]
    down_rows, down_cols = sd_ref.shape

    def tp_rows(size):
        return pl.ds(pl.multiple_of(tp * size, size), size)

    barrier, arrivals = greet((("fs", range(1, n)), ("tp", range(1, m))))
    widened = tok_ref[...].astype(jnp.float32)
    scale = lax.rsqrt(jnp.mean(widened * widened, axis=1, keepdims=True) + EPSILON)
    all_ref[pl.ds(0, rows), :] = (widened * scale).astype(jnp.bfloat16)
    scores = sc_ref[...]
    meta_ref[0, pl.ds(0, picks), :] = ids_ref[...].astype(jnp.float32)
    meta_ref[0, pl.ds(picks, picks), :] = route_scale * scores / jnp.sum(scores, axis=0, keepdims=True)
    gain = gain_ref[...]
    sgu_ref[0] = (gain * sg_ref[...]).astype(jnp.bfloat16)
    sgu_ref[1] = (gain * su_ref[...]).astype(jnp.bfloat16)
    sd_ref[...] = sd32_ref[...].astype(jnp.bfloat16)
    hgu_ref[:, tp_rows(cols_f), :] = sgu_ref[...]
    hd_ref[:, tp_rows(down_cols)] = sd_ref[...]
    pl.semaphore_wait(barrier, arrivals)

    step_rows = rows // AG_PIECES

    def ring(k, p):
        src = max(k - 2, 0)
        upward = k % 2 == 1
        if k == n - 1 and p >= AG_PIECES // 2:
            src, upward = k - 1, False
        return remote(
            all_ref.at[pl.ds(src * rows + p * step_rows, step_rows), :],
            all_ref.at[pl.ds(k * rows + p * step_rows, step_rows), :],
            ag_send.at[k, p], ag_recv.at[k, p], "fs", above if upward else below,
        )

    def ring_meta(k):
        return remote(
            meta_ref.at[max(k - 2, 0)], meta_ref.at[k], meta_send.at[k], meta_recv.at[k],
            "fs", above if k % 2 == 1 else below,
        )

    def gather_gu(q):
        return remote(
            sgu_ref, hgu_ref.at[:, tp_rows(cols_f), :], gu_send.at[q - 1], gu_recv.at[q - 1], "tp", lax.rem(tp + q, m)
        )

    def gather_sd(q):
        return remote(
            sd_ref, hd_ref.at[:, tp_rows(down_cols)], sd_send.at[q - 1], sd_recv.at[q - 1], "tp", lax.rem(tp + q, m)
        )

    def slice_gs(r):
        peer = lax.rem(z + r, n)
        return remote(
            hgu_ref.at[:, pl.ds(pl.multiple_of(peer * own_h, own_h), own_h), :],
            gs_ref.at[:, :, pl.ds(pl.multiple_of(z * deep, deep), deep)],
            gs_send.at[r - 1], gs_recv.at[r - 1], "fs", peer,
        )

    kinds = (
        (wg_ref, mg_ref, fg_ref), (wu_ref, mu_ref, fu_ref), (wd_ref, md_ref, fd_ref),
    )

    def mid_place(kind, first, count):
        if kind < 2:
            return (slice(None), slice(None), pl.ds(first * deep, count * deep))
        return (slice(None), pl.ds(first * down_rows, count * down_rows), slice(None))

    def weight_z(at, kind):
        peer = lax.rem(z + n - offset_of(order[at]), n)
        src, mid, _ = kinds[kind]
        w = bundle_of[at]
        return remote(
            src.at[peer], mid.at[mid_place(kind, at, 1)], wz_send.at[w, kind], wz_recv.at[w, kind], "fs", peer
        )

    def weight_z_all(w, kind):
        first, count = bundles[w]
        first, count = max(1, first), count - (first == 0)
        _, mid, _ = kinds[kind]
        return remote(
            mid.at[mid_place(kind, first, count)], mid.at[mid_place(kind, first, count)],
            wz_send.at[w, kind], wz_recv.at[w, kind], "fs", above,
        )

    def piece(w, kind, who):
        first, count = bundles[w]
        if kind < 2:
            return who, slice(None), pl.ds(first * deep, count * deep)
        return who, pl.ds(first * down_rows, count * down_rows), slice(None)

    def landing(w, kind, where):
        first, count = bundles[w]
        if kind < 2:
            return where, pl.ds(first * deep, count * deep)
        return pl.ds(first * down_rows, count * down_rows), where

    def weight_x(w, q, kind):
        peer = lax.rem(tp + q, m)
        _, mid, final = kinds[kind]
        where = tp_rows(cols_f if kind < 2 else down_cols)
        return remote(
            mid.at[piece(w, kind, peer)], final.at[landing(w, kind, where)],
            wx_send.at[w, kind], wx_recv.at[w, kind], "tp", peer,
        )

    def weight_x_all(w, kind):
        _, _, final = kinds[kind]
        where = pl.ds(0, (m - 1) * (cols_f if kind < 2 else down_cols))
        return remote(
            final.at[landing(w, kind, where)], final.at[landing(w, kind, where)],
            wx_send.at[w, kind], wx_recv.at[w, kind], "tp", lax.rem(tp + 1, m),
        )

    def of(who):
        return pl.ds(pl.multiple_of(who * slots, slots), slots)

    most = pl.ds(0, (m - 1) * slots)

    def exchange(g, q):
        peer = lax.rem(tp + q, m)
        return remote(stage_ref.at[g, :, of(peer)], x_ref.at[g, :, of(tp)], x_send.at[g], x_recv.at[g], "tp", peer)

    def exchange_all(g):
        return remote(
            stage_ref.at[g, :, most], x_ref.at[g, :, most], x_send.at[g], x_recv.at[g], "tp", lax.rem(tp + 1, m)
        )

    def answer(g, c, q):
        peer = lax.rem(tp + q, m)
        return remote(
            stage_ref.at[g, c, of(peer)], rv_ref.at[g, c, of(tp)], y_send.at[g, c], y_recv.at[g, c], "tp", peer
        )

    def answer_all(g, c):
        return remote(
            stage_ref.at[g, c, most], rv_ref.at[g, c, most], y_send.at[g, c], y_recv.at[g, c], "tp", lax.rem(tp + 1, m)
        )

    span = n // LOADS
    loads = ((eg_ref, eg32_ref), (eu_ref, eu32_ref), (ed_ref, ed32_ref))

    def load(i, kind):
        src, dst = loads[kind]
        return pltpu.make_async_copy(src.at[pl.ds(i * span, span)], dst.at[i % 2], load_sem.at[i % 2, kind])

    for kind in range(3):
        load(0, kind).start()
    for k in (1, 2):
        ring_meta(k).start()
        for p in range(AG_PIECES):
            ring(k, p).start()
    for q in range(1, m):
        gather_gu(q).start()
        gather_sd(q).start()
    for i in range(LOADS):
        for kind in range(3):
            if i + 1 < LOADS:
                load(i + 1, kind).start()
            load(i, kind).wait()
        some = pl.ds(i * span, span)
        wg_ref[some] = (gain * eg32_ref[i % 2]).astype(jnp.bfloat16)
        wu_ref[some] = (gain * eu32_ref[i % 2]).astype(jnp.bfloat16)
        wd_ref[some] = ed32_ref[i % 2].astype(jnp.bfloat16)
    for kind, (src, mid, _) in enumerate(kinds):
        mid[mid_place(kind, 0, 1)] = src[z]
    for q in range(1, m):
        gather_gu(q).wait_recv()
    for r in range(1, n):
        slice_gs(r).start()
    gs_ref[:, :, pl.ds(pl.multiple_of(z * deep, deep), deep)] = hgu_ref[
        :, pl.ds(pl.multiple_of(z * own_h, own_h), own_h), :
    ]

    before = lax.broadcasted_iota(jnp.int32, (rows, rows), 0) < lax.broadcasted_iota(jnp.int32, (rows, rows), 1)
    before = before.astype(jnp.float32).astype(jnp.bfloat16)
    served = (lax.broadcasted_iota(jnp.int32, (m, rows), 0) + m * z).astype(jnp.float32)
    places = lax.broadcasted_iota(jnp.int32, (slots, rows), 0).astype(jnp.float32)

    def select(g):
        for b in range(GROUP):
            k = g * GROUP + b
            meta = meta_ref[k]
            chosen = jnp.zeros((m, rows), jnp.float32)
            weight = jnp.zeros((m, rows), jnp.float32)
            for j in range(picks):
                hit = meta[j : j + 1, :] == served
                chosen = chosen + hit.astype(jnp.float32)
                weight = weight + jnp.where(hit, meta[picks + j : picks + j + 1, :], 0.0)
            rank = jnp.dot(chosen.astype(jnp.bfloat16), before, preferred_element_type=jnp.float32)
            code = jnp.where(chosen > 0.0, rank, ABSENT)
            cw_ref[k, pl.ds(0, m), :] = code
            cw_ref[k, pl.ds(m, m), :] = weight
            for q in range(m):
                hot = (jnp.broadcast_to(code[q : q + 1, :], (slots, rows)) + float(cap * b)) == places
                pick_ref[pl.ds(q * slots, slots), pl.ds(b * rows, rows)] = hot.astype(jnp.float32).astype(jnp.bfloat16)

        @pl.loop(0, parts)
        def _(c):
            cols = pl.ds(pl.multiple_of(c * wide, wide), wide)
            taken = jnp.dot(
                pick_ref[...], all_ref[pl.ds(g * GROUP * rows, GROUP * rows), cols],
                preferred_element_type=jnp.float32,
            ).astype(jnp.bfloat16)
            stage_ref[g, c] = taken
            x_ref[g, c, of(tp), :] = stage_ref[g, c, of(tp), :]

        for q in range(1, m):
            exchange(g, q).start()

    moved_on = []

    def move_on(w):
        moved_on.append(w)
        for kind in range(3):
            weight_z_all(w, kind).wait_recv()
        for q in range(1, m):
            for kind in range(3):
                weight_x(w, q, kind).start()
        for kind, (_, mid, final) in enumerate(kinds):
            where = tp_rows(cols_f if kind < 2 else down_cols)
            final[landing(w, kind, where)] = mid[piece(w, kind, tp)]

    issue = {}
    for at in range(1, n):
        issue.setdefault(max(1, min(n - 3, 1 + 2 * (at // 2))), []).append(at)
    for k in range(1, n):
        ring_meta(k).wait_recv()
        if k + 2 < n:
            ring_meta(k + 2).start()
        for p in range(AG_PIECES):
            ring(k, p).wait_recv()
            onward = k + 2 if k + 2 < n - 1 or (k + 2 == n - 1 and p < AG_PIECES // 2) else None
            if k == n - 2 and p >= AG_PIECES // 2:
                onward = n - 1
            if onward is not None:
                ring(onward, p).start()
        for at in issue.get(k, ()):
            for kind in range(3):
                weight_z(at, kind).start()
        if k % GROUP == GROUP - 1:
            select(k // GROUP)
            if groups > 2 and k // GROUP >= groups - 2:
                move_on(k // GROUP - groups + 2)

    for r in range(1, n):
        slice_gs(r).wait_recv()
    for g in range(groups):
        some = pl.ds(g * GROUP * rows, GROUP * rows)
        both = lax.dot_general(
            all_ref[some, :], gs_ref[...].reshape(2 * own_h, width), (((1,), (1,)), ((), ())),
            preferred_element_type=jnp.float32,
        )
        gate, upper = both[:, :own_h], both[:, own_h:]
        c_ref[g, :, pl.ds(lanes, own_h)] = (gate / (1.0 + jnp.exp(-gate)) * upper).astype(jnp.bfloat16)
        turned = jnp.transpose(cw_ref[pl.ds(g * GROUP, GROUP)].reshape(GROUP * 2 * m, rows)).astype(jnp.bfloat16)
        for b in range(GROUP):
            code = jnp.dot(turned, ecode_ref[b], preferred_element_type=jnp.float32)
            value = jnp.dot(turned, ew_ref[b], preferred_element_type=jnp.float32)
            hit = (code + float(cap * b)) == place_ref[...]
            c_ref[g, pl.ds(b * rows, rows), pl.ds(0, lanes)] = jnp.where(hit, value, 0.0).astype(jnp.bfloat16)
    for q in range(1, m):
        gather_sd(q).wait_recv()
    for g in range(groups):
        for c in range(parts):
            rv_ref[g, c, pl.ds(lanes, own_h), :] = hd_ref[:, pl.ds(c * wide, wide)]

    def settle(w):
        for kind in range(3):
            weight_x_all(w, kind).wait_recv()
        for at in range(bundles[w][0], sum(bundles[w])):
            source = lax.rem(z + n + offset_of(order[at]), n)
            there = pl.ds(pl.multiple_of(source * deep, deep), deep)
            gate_ref[there, :] = jnp.transpose(fg_ref[:, pl.ds(at * deep, deep)])
            up_ref[there, :] = jnp.transpose(fu_ref[:, pl.ds(at * deep, deep)])
            down_ref[pl.ds(pl.multiple_of(source * down_rows, down_rows), down_rows), :] = fd_ref[
                pl.ds(at * down_rows, down_rows), :
            ]

    settled = 0
    for w in range(len(bundles)):
        if w not in moved_on:
            while settled < w - 1:
                settle(settled)
                settled += 1
            move_on(w)
    for w in range(settled, len(bundles)):
        settle(w)

    for g in range(groups):
        exchange_all(g).wait_send()
        exchange_all(g).wait_recv()

    def experts(first, count):
        @pl.loop(0, count)
        def _(i):
            g = first - i
            gate = jnp.zeros((lanes, gate_ref.shape[1]), jnp.float32)
            upper = jnp.zeros((lanes, gate_ref.shape[1]), jnp.float32)
            for c in range(parts):
                x = x_ref[g, c]
                deep_rows = pl.ds(c * wide, wide)
                gate += jnp.dot(x, gate_ref[deep_rows, :], preferred_element_type=jnp.float32)
                upper += jnp.dot(x, up_ref[deep_rows, :], preferred_element_type=jnp.float32)
            hidden = (gate / (1.0 + jnp.exp(-gate)) * upper).astype(jnp.bfloat16)

            @pl.loop(0, parts)
            def _(c):
                cols = pl.ds(pl.multiple_of(c * wide, wide), wide)
                y = jnp.dot(hidden, down_ref[:, cols], preferred_element_type=jnp.float32)
                stage_ref[g, c] = y.astype(jnp.bfloat16)
                rv_ref[g, c, of(tp), :] = stage_ref[g, c, of(tp), :]
                for q in range(1, m):
                    answer(g, c, q).start()

    def combine(g, c):
        answer_all(g, c).wait_recv()
        d_ref[c] = jnp.dot(c_ref[g], rv_ref[g, c], preferred_element_type=jnp.float32)

    def share(offset, c):
        return d_ref[c, pl.ds((slot_of(offset) % GROUP) * rows, rows), :]

    def hop(sign, r, c):
        if sign > 0:
            return remote(pst_ref.at[r % 2, c], pin_ref.at[r - 1, c],
                          p_send.at[r - 1, c], p_recv.at[r - 1, c], "fs", above)
        return remote(mst_ref.at[r % 2, c], min_ref.at[r - 1, c],
                      m_send.at[r - 1, c], m_recv.at[r - 1, c], "fs", below)

    cut = (parts + 1) // 2

    def forward(sign, r, c, low):
        last = half if (sign < 0) == low else half - 1
        total = share(sign * r if r < half else -half, c)
        if r < last:
            hop(sign, r + 1, c).wait_recv()
            total = total + (pin_ref if sign > 0 else min_ref)[r, c].astype(jnp.float32)
        if r + 2 <= last:
            hop(sign, r + 2, c).wait_send()
        (pst_ref if sign > 0 else mst_ref)[r % 2, c] = total.astype(jnp.bfloat16)
        hop(sign, r, c).start()

    def steps(i, low):
        if i == 0:
            return ((-1, half), (1, half - 1)) if low else ((1, half), (-1, half - 1))
        if i == 1 and not low:
            return ((1, half - 1), (1, half - 2))
        return (-1, half - i), (1, half - 1 - i)

    early = min(2, groups)
    experts(groups - 1, early)
    for i in range(half):
        g = groups - 1 - i // 2
        for low, first, end in ((True, 0, cut), (False, cut, parts)):
            if first == end:
                continue

            @pl.loop(first, end)
            def _(c):
                if i == 0:
                    combine(g, c)
                for at, (sign, r) in enumerate(steps(i, low)):
                    if r > 0 and not (at == 1 and i == 1 and not low):
                        forward(sign, r, c, low)

        for low, first, end in ((True, 0, cut), (False, cut, parts)):
            late = i == 1 and not low and half > 2
            if first == end or not (late or (i % 2 == 1 and g > 0)):
                continue

            @pl.loop(first, end)
            def _(c):
                if late:
                    forward(*steps(i, low)[1], c, low)
                if i % 2 == 1 and g > 0:
                    combine(g - 1, c)

        if i < groups - early:
            experts(groups - 1 - early - i, 1)

    @pl.loop(0, parts)
    def _(c):
        hop(1, 1, c).wait_recv()
        hop(-1, 1, c).wait_recv()
        total = share(0, c) + pin_ref[0, c].astype(jnp.float32) + min_ref[0, c].astype(jnp.float32)
        out_ref[:, pl.ds(pl.multiple_of(c * wide, wide), wide)] = total.astype(jnp.bfloat16)

    for c in range(parts):
        for sign in (-1, 1):
            for r in range(1, min(2, half if (sign < 0) == (c < cut) else half - 1) + 1):
                hop(sign, r, c).wait_send()
        for g in range(groups):
            answer_all(g, c).wait_send()
    for q in range(1, m):
        gather_gu(q).wait_send()
        gather_sd(q).wait_send()
    for r in range(1, n):
        slice_gs(r).wait_send()
    for k in range(1, n):
        ring_meta(k).wait_send()
        for p in range(AG_PIECES):
            ring(k, p).wait_send()
    for w in range(len(bundles)):
        for kind in range(3):
            weight_z_all(w, kind).wait_send()
            weight_x_all(w, kind).wait_send()


def hand_on(
    mixed_ref, gate_ref, up_ref, down_ref, hgu_ref, hd_ref,
    mixed_out, gate_out, up_out, down_out, shared_gate_out, shared_up_out, shared_down_out,
):
    mixed_out[...] = mixed_ref[...]
    gate_out[0] = gate_ref[...]
    up_out[0] = up_ref[...]
    down_out[0] = down_ref[...]
    shared_gate_out[...] = jnp.transpose(hgu_ref[0])
    shared_up_out[...] = jnp.transpose(hgu_ref[1])
    shared_down_out[...] = hd_ref[...]


def on_device(
    tokens, route_ids, route_scores, norm_gain,
    expert_gate, expert_up, expert_down, shared_gate, shared_up, shared_down,
):
    n = lax.axis_size("fs")
    m = lax.axis_size("tp")
    experts = n * m
    rows, width = tokens.shape
    picks = route_ids.shape[1]
    cap = 3 * rows * picks // (2 * experts)
    slots = GROUP * cap
    lanes = m * slots
    groups = n // GROUP
    half = n // 2
    bf16, f32 = jnp.bfloat16, jnp.float32
    dma = pltpu.SemaphoreType.DMA
    wide = min(512, width)
    parts = width // wide

    deep, cols_f = expert_gate.shape[1:]
    down_rows, down_cols = expert_down.shape[1:]
    hidden = m * cols_f
    own_h = hidden // n

    def turned(weight):
        return jnp.swapaxes(weight, 1, 2).reshape(n, m, cols_f, deep)

    lane = np.arange(lanes)
    row = np.arange(GROUP * 2 * m)
    block = np.arange(GROUP)

    def expand(first):
        wanted = block[:, None, None] * 2 * m + first + (lane // slots)[None, None, :]
        return jnp.asarray((row[None, :, None] == wanted).astype(np.float32), bf16)

    place = jnp.asarray((lane % slots)[None, :].astype(np.float32))
    held = pl.BlockSpec(memory_space=pl.ANY)
    results = pl.pallas_call(
        functools.partial(kernel, n, m, cap),
        out_shape=(
            jax.ShapeDtypeStruct((rows, width), bf16),
            jax.ShapeDtypeStruct((width, hidden), bf16),
            jax.ShapeDtypeStruct((width, hidden), bf16),
            jax.ShapeDtypeStruct((hidden, width), bf16),
            jax.ShapeDtypeStruct((2, hidden, deep), bf16),
            jax.ShapeDtypeStruct((down_rows, width), bf16),
        ),
        in_specs=[VMEM] * 7 + [held] * 3 + [VMEM] * 3,
        out_specs=(VMEM,) * 6,
        scratch_shapes=[
            pltpu.VMEM((n * rows, width), bf16),
            pltpu.VMEM((n, 2 * picks, rows), f32),
            pltpu.VMEM((n, 2 * m, rows), f32),
            pltpu.VMEM((groups, parts, lanes, wide), bf16),
            pltpu.VMEM((groups, parts, lanes, wide), bf16),
            pltpu.VMEM((groups, parts, lanes + own_h, wide), bf16),
            pltpu.VMEM((lanes, GROUP * rows), bf16),
            pltpu.VMEM((2, own_h, width), bf16),
            pltpu.VMEM((2, cols_f, deep), bf16),
            pltpu.VMEM((down_rows, down_cols), bf16),
            pltpu.VMEM((2, n // LOADS, m, cols_f, deep), f32),
            pltpu.VMEM((2, n // LOADS, m, cols_f, deep), f32),
            pltpu.VMEM((2, n // LOADS, m, down_rows, down_cols), f32),
            pltpu.VMEM((n, m, cols_f, deep), bf16),
            pltpu.VMEM((n, m, cols_f, deep), bf16),
            pltpu.VMEM((n, m, down_rows, down_cols), bf16),
            pltpu.VMEM((m, cols_f, width), bf16),
            pltpu.VMEM((m, cols_f, width), bf16),
            pltpu.VMEM((m, n * down_rows, down_cols), bf16),
            pltpu.VMEM((hidden, width), bf16),
            pltpu.VMEM((hidden, width), bf16),
            pltpu.VMEM((hidden, width), bf16),
            pltpu.VMEM((groups, GROUP * rows, lanes + own_h), bf16),
            pltpu.VMEM((parts, GROUP * rows, wide), f32),
            pltpu.VMEM((half, parts, rows, wide), bf16),
            pltpu.VMEM((half, parts, rows, wide), bf16),
            pltpu.VMEM((2, parts, rows, wide), bf16),
            pltpu.VMEM((2, parts, rows, wide), bf16),
            dma((n, AG_PIECES)), dma((n, AG_PIECES)), dma((n,)), dma((n,)),
            dma((groups,)), dma((groups,)), dma((groups, parts)), dma((groups, parts)),
            dma((m - 1,)), dma((m - 1,)), dma((m - 1,)), dma((m - 1,)), dma((n - 1,)), dma((n - 1,)),
            dma((2, 3)), *[dma((groups + 1, 3))] * 4,
            *[dma((half, parts))] * 4,
        ],
        compiler_params=pltpu.CompilerParams(
            collective_id=0, has_side_effects=True, vmem_limit_bytes=63 * 1024 * 1024,
        ),
        cost_estimate=pl.CostEstimate(flops=100_000_000_000, bytes_accessed=30_000_000, transcendentals=0),
        name="hand_over",
    )(
        tokens, route_ids.T, route_scores.T, norm_gain[None, :], shared_gate.T, shared_up.T, shared_down,
        turned(expert_gate), turned(expert_up), expert_down.reshape(n, m, down_rows, down_cols),
        expand(0), expand(m), place,
    )
    whole = jax.ShapeDtypeStruct((1, width, hidden), bf16)
    held_up = jax.ShapeDtypeStruct((deep, hidden), bf16)
    return pl.pallas_call(
        hand_on,
        out_shape=(
            jax.ShapeDtypeStruct((rows, width), bf16), whole, whole, jax.ShapeDtypeStruct((1, hidden, width), bf16),
            held_up, held_up, jax.ShapeDtypeStruct((down_rows, width), bf16),
        ),
        in_specs=[VMEM] * 6,
        out_specs=(VMEM,) * 7,
        cost_estimate=pl.CostEstimate(flops=1_000_000, bytes_accessed=8_000_000, transcendentals=0),
        name="hand_on",
    )(*results)


def solution(mesh):
    return jax.shard_map(
        on_device,
        mesh=mesh,
        in_specs=(
            P(("grp", "fs", "tp"), None),
            P(("grp", "fs", "tp"), None),
            P(("grp", "fs", "tp"), None),
            P("fs"),
            P(None, "fs", "tp"),
            P(None, "fs", "tp"),
            P(None, "fs", "tp"),
            P("fs", "tp"),
            P("fs", "tp"),
            P("fs", "tp"),
        ),
        out_specs=(
            P(("grp", "fs", "tp"), None),
            P(("grp", "fs", "tp"), None, None),
            P(("grp", "fs", "tp"), None, None),
            P(("grp", "fs", "tp"), None, None),
            P(("grp", "fs"), None),
            P(("grp", "fs"), None),
            P(("grp", "fs"), None),
        ),
        check_vma=False,
    )
```

```python
import functools

import jax
import jax.numpy as jnp
import numpy as np
from jax import lax
from jax.experimental import pallas as pl
from jax.experimental.pallas import tpu as pltpu
from jax.sharding import PartitionSpec as P

EPSILON = 1e-06
route_scale = 2.5
ABSENT = -1024.0
MESH = pl.DeviceIdType.MESH
GROUP = 4
AG_PIECES = 2
LOADS = 4
VMEM = pl.BlockSpec(memory_space=pltpu.VMEM)


def slot_of(offset):
    return 2 * offset if offset >= 0 else -2 * offset - 1


def greet(names_and_counts):
    barrier = pltpu.get_barrier_semaphore()
    total = 0
    for name, steps in names_and_counts:
        size = lax.axis_size(name)
        me = lax.axis_index(name)
        for step in steps:
            peer = lax.rem(me + step + size, size)
            pl.semaphore_signal(barrier, inc=1, device_id={name: peer}, device_id_type=MESH)
            total += 1
    return barrier, total


def remote(src, dst, send, recv, name, peer):
    return pltpu.make_async_remote_copy(
        src_ref=src, dst_ref=dst, send_sem=send, recv_sem=recv,
        device_id={name: peer}, device_id_type=MESH,
    )


def offset_of(slot):
    return slot // 2 if slot % 2 == 0 else -((slot + 1) // 2)


def weight_order(n):
    order, far, near = [0, n - 1], n - 2, 1
    while near <= far:
        order.append(far)
        if near < far:
            order.append(near)
        far, near = far - 1, near + 1
    return order


def kernel(
    n, m, cap, tok_ref, ids_ref, sc_ref, gain_ref, sg_ref, su_ref, sd32_ref, eg_ref, eu_ref, ed_ref,
    ecode_ref, ew_ref, place_ref,
    out_ref, gate_ref, up_ref, down_ref, hgu_ref, hd_ref,
    all_ref, meta_ref, cw_ref, stage_ref, x_ref, rv_ref, pick_ref, gs_ref,
    sgu_ref, sd_ref, eg32_ref, eu32_ref, ed32_ref, wg_ref, wu_ref, wd_ref,
    mg_ref, mu_ref, md_ref, fg_ref, fu_ref, fd_ref, c_ref, d_ref, pin_ref, min_ref, pst_ref, mst_ref,
    ag_send, ag_recv, meta_send, meta_recv, x_send, x_recv, y_send, y_recv,
    gu_send, gu_recv, sd_send, sd_recv, gs_send, gs_recv,
    load_sem, wz_send, wz_recv, wx_send, wx_recv, p_send, p_recv, m_send, m_recv,
):
    z, tp = lax.axis_index("fs"), lax.axis_index("tp")
    rows, width = tok_ref.shape
    picks = ids_ref.shape[0]
    above, below = lax.rem(z + 1, n), lax.rem(z + n - 1, n)
    parts, wide = stage_ref.shape[1], stage_ref.shape[3]
    slots = GROUP * cap
    lanes = m * slots
    half, groups = n // 2, n // GROUP
    cols_f, deep = sgu_ref.shape[1:]
    order = weight_order(n)
    bundles = [(first, GROUP) for first in range(0, n - GROUP, GROUP)] + [(n - GROUP, GROUP - 1), (n - 1, 1)]
    bundle_of = [w for w, (_, count) in enumerate(bundles) for _ in range(count)]
    own_h = gs_ref.shape[1]
    down_rows, down_cols = sd_ref.shape

    def tp_rows(size):
        return pl.ds(pl.multiple_of(tp * size, size), size)

    barrier, arrivals = greet((("fs", range(1, n)), ("tp", range(1, m))))
    widened = tok_ref[...].astype(jnp.float32)
    scale = lax.rsqrt(jnp.mean(widened * widened, axis=1, keepdims=True) + EPSILON)
    all_ref[pl.ds(0, rows), :] = (widened * scale).astype(jnp.bfloat16)
    scores = sc_ref[...]
    meta_ref[0, pl.ds(0, picks), :] = ids_ref[...].astype(jnp.float32)
    meta_ref[0, pl.ds(picks, picks), :] = route_scale * scores / jnp.sum(scores, axis=0, keepdims=True)
    gain = gain_ref[...]
    sgu_ref[0] = (gain * sg_ref[...]).astype(jnp.bfloat16)
    sgu_ref[1] = (gain * su_ref[...]).astype(jnp.bfloat16)
    sd_ref[...] = sd32_ref[...].astype(jnp.bfloat16)
    hgu_ref[:, tp_rows(cols_f), :] = sgu_ref[...]
    hd_ref[:, tp_rows(down_cols)] = sd_ref[...]
    pl.semaphore_wait(barrier, arrivals)

    step_rows = rows // AG_PIECES

    def ring(k, p):
        src = max(k - 2, 0)
        upward = k % 2 == 1
        if k == n - 1 and p >= AG_PIECES // 2:
            src, upward = k - 1, False
        return remote(
            all_ref.at[pl.ds(src * rows + p * step_rows, step_rows), :],
            all_ref.at[pl.ds(k * rows + p * step_rows, step_rows), :],
            ag_send.at[k, p], ag_recv.at[k, p], "fs", above if upward else below,
        )

    def ring_meta(k):
        return remote(
            meta_ref.at[max(k - 2, 0)], meta_ref.at[k], meta_send.at[k], meta_recv.at[k],
            "fs", above if k % 2 == 1 else below,
        )

    def gather_gu(q):
        return remote(
            sgu_ref, hgu_ref.at[:, tp_rows(cols_f), :], gu_send.at[q - 1], gu_recv.at[q - 1], "tp", lax.rem(tp + q, m)
        )

    def gather_sd(q):
        return remote(
            sd_ref, hd_ref.at[:, tp_rows(down_cols)], sd_send.at[q - 1], sd_recv.at[q - 1], "tp", lax.rem(tp + q, m)
        )

    def slice_gs(r):
        peer = lax.rem(z + r, n)
        return remote(
            hgu_ref.at[:, pl.ds(pl.multiple_of(peer * own_h, own_h), own_h), :],
            gs_ref.at[:, :, pl.ds(pl.multiple_of(z * deep, deep), deep)],
            gs_send.at[r - 1], gs_recv.at[r - 1], "fs", peer,
        )

    kinds = (
        (wg_ref, mg_ref, fg_ref), (wu_ref, mu_ref, fu_ref), (wd_ref, md_ref, fd_ref),
    )

    def mid_place(kind, first, count):
        if kind < 2:
            return (slice(None), slice(None), pl.ds(first * deep, count * deep))
        return (slice(None), pl.ds(first * down_rows, count * down_rows), slice(None))

    def weight_z(at, kind):
        peer = lax.rem(z + n - offset_of(order[at]), n)
        src, mid, _ = kinds[kind]
        w = bundle_of[at]
        return remote(
            src.at[peer], mid.at[mid_place(kind, at, 1)], wz_send.at[w, kind], wz_recv.at[w, kind], "fs", peer
        )

    def weight_z_all(w, kind):
        first, count = bundles[w]
        first, count = max(1, first), count - (first == 0)
        _, mid, _ = kinds[kind]
        return remote(
            mid.at[mid_place(kind, first, count)], mid.at[mid_place(kind, first, count)],
            wz_send.at[w, kind], wz_recv.at[w, kind], "fs", above,
        )

    def piece(w, kind, who):
        first, count = bundles[w]
        if kind < 2:
            return who, slice(None), pl.ds(first * deep, count * deep)
        return who, pl.ds(first * down_rows, count * down_rows), slice(None)

    def landing(w, kind, where):
        first, count = bundles[w]
        if kind < 2:
            return where, pl.ds(first * deep, count * deep)
        return pl.ds(first * down_rows, count * down_rows), where

    def weight_x(w, q, kind):
        peer = lax.rem(tp + q, m)
        _, mid, final = kinds[kind]
        where = tp_rows(cols_f if kind < 2 else down_cols)
        return remote(
            mid.at[piece(w, kind, peer)], final.at[landing(w, kind, where)],
            wx_send.at[w, kind], wx_recv.at[w, kind], "tp", peer,
        )

    def weight_x_all(w, kind):
        _, _, final = kinds[kind]
        where = pl.ds(0, (m - 1) * (cols_f if kind < 2 else down_cols))
        return remote(
            final.at[landing(w, kind, where)], final.at[landing(w, kind, where)],
            wx_send.at[w, kind], wx_recv.at[w, kind], "tp", lax.rem(tp + 1, m),
        )

    def of(who):
        return pl.ds(pl.multiple_of(who * slots, slots), slots)

    most = pl.ds(0, (m - 1) * slots)

    def exchange(g, q):
        peer = lax.rem(tp + q, m)
        return remote(stage_ref.at[g, :, of(peer)], x_ref.at[g, :, of(tp)], x_send.at[g], x_recv.at[g], "tp", peer)

    def exchange_all(g):
        return remote(
            stage_ref.at[g, :, most], x_ref.at[g, :, most], x_send.at[g], x_recv.at[g], "tp", lax.rem(tp + 1, m)
        )

    def answer(g, c, q):
        peer = lax.rem(tp + q, m)
        return remote(
            stage_ref.at[g, c, of(peer)], rv_ref.at[g, c, of(tp)], y_send.at[g, c], y_recv.at[g, c], "tp", peer
        )

    def answer_all(g, c):
        return remote(
            stage_ref.at[g, c, most], rv_ref.at[g, c, most], y_send.at[g, c], y_recv.at[g, c], "tp", lax.rem(tp + 1, m)
        )

    span = n // LOADS
    loads = ((eg_ref, eg32_ref), (eu_ref, eu32_ref), (ed_ref, ed32_ref))

    def load(i, kind):
        src, dst = loads[kind]
        return pltpu.make_async_copy(src.at[pl.ds(i * span, span)], dst.at[i % 2], load_sem.at[i % 2, kind])

    for kind in range(3):
        load(0, kind).start()
    for k in (1, 2):
        ring_meta(k).start()
        for p in range(AG_PIECES):
            ring(k, p).start()
    for q in range(1, m):
        gather_gu(q).start()
        gather_sd(q).start()
    for i in range(LOADS):
        for kind in range(3):
            if i + 1 < LOADS:
                load(i + 1, kind).start()
            load(i, kind).wait()
        some = pl.ds(i * span, span)
        wg_ref[some] = (gain * eg32_ref[i % 2]).astype(jnp.bfloat16)
        wu_ref[some] = (gain * eu32_ref[i % 2]).astype(jnp.bfloat16)
        wd_ref[some] = ed32_ref[i % 2].astype(jnp.bfloat16)
    for kind, (src, mid, _) in enumerate(kinds):
        mid[mid_place(kind, 0, 1)] = src[z]
    for q in range(1, m):
        gather_gu(q).wait_recv()
    for r in range(1, n):
        slice_gs(r).start()
    gs_ref[:, :, pl.ds(pl.multiple_of(z * deep, deep), deep)] = hgu_ref[
        :, pl.ds(pl.multiple_of(z * own_h, own_h), own_h), :
    ]

    before = lax.broadcasted_iota(jnp.int32, (rows, rows), 0) < lax.broadcasted_iota(jnp.int32, (rows, rows), 1)
    before = before.astype(jnp.float32).astype(jnp.bfloat16)
    served = (lax.broadcasted_iota(jnp.int32, (m, rows), 0) + m * z).astype(jnp.float32)
    places = lax.broadcasted_iota(jnp.int32, (slots, rows), 0).astype(jnp.float32)

    def select(g):
        for b in range(GROUP):
            k = g * GROUP + b
            meta = meta_ref[k]
            chosen = jnp.zeros((m, rows), jnp.float32)
            weight = jnp.zeros((m, rows), jnp.float32)
            for j in range(picks):
                hit = meta[j : j + 1, :] == served
                chosen = chosen + hit.astype(jnp.float32)
                weight = weight + jnp.where(hit, meta[picks + j : picks + j + 1, :], 0.0)
            rank = jnp.dot(chosen.astype(jnp.bfloat16), before, preferred_element_type=jnp.float32)
            code = jnp.where(chosen > 0.0, rank, ABSENT)
            cw_ref[k, pl.ds(0, m), :] = code
            cw_ref[k, pl.ds(m, m), :] = weight
            for q in range(m):
                hot = (jnp.broadcast_to(code[q : q + 1, :], (slots, rows)) + float(cap * b)) == places
                pick_ref[pl.ds(q * slots, slots), pl.ds(b * rows, rows)] = hot.astype(jnp.float32).astype(jnp.bfloat16)

        @pl.loop(0, parts)
        def _(c):
            cols = pl.ds(pl.multiple_of(c * wide, wide), wide)
            taken = jnp.dot(
                pick_ref[...], all_ref[pl.ds(g * GROUP * rows, GROUP * rows), cols],
                preferred_element_type=jnp.float32,
            ).astype(jnp.bfloat16)
            stage_ref[g, c] = taken
            x_ref[g, c, of(tp), :] = stage_ref[g, c, of(tp), :]

        for q in range(1, m):
            exchange(g, q).start()

    moved_on = []

    def move_on(w):
        moved_on.append(w)
        for kind in range(3):
            weight_z_all(w, kind).wait_recv()
        for q in range(1, m):
            for kind in range(3):
                weight_x(w, q, kind).start()
        for kind, (_, mid, final) in enumerate(kinds):
            where = tp_rows(cols_f if kind < 2 else down_cols)
            final[landing(w, kind, where)] = mid[piece(w, kind, tp)]

    issue = {}
    for at in range(1, n):
        issue.setdefault(max(1, min(n - 2, 1 + 2 * (at // 2))), []).append(at)
    for k in range(1, n):
        ring_meta(k).wait_recv()
        if k + 2 < n:
            ring_meta(k + 2).start()
        for p in range(AG_PIECES):
            ring(k, p).wait_recv()
            onward = k + 2 if k + 2 < n - 1 or (k + 2 == n - 1 and p < AG_PIECES // 2) else None
            if k == n - 2 and p >= AG_PIECES // 2:
                onward = n - 1
            if onward is not None:
                ring(onward, p).start()
        for at in issue.get(k, ()):
            for kind in range(3):
                weight_z(at, kind).start()
        if k % GROUP == GROUP - 1:
            select(k // GROUP)
            if groups > 2 and k // GROUP >= groups - 2:
                move_on(k // GROUP - groups + 2)

    for r in range(1, n):
        slice_gs(r).wait_recv()
    for g in range(groups):
        some = pl.ds(g * GROUP * rows, GROUP * rows)
        both = lax.dot_general(
            all_ref[some, :], gs_ref[...].reshape(2 * own_h, width), (((1,), (1,)), ((), ())),
            preferred_element_type=jnp.float32,
        )
        gate, upper = both[:, :own_h], both[:, own_h:]
        c_ref[g, :, pl.ds(lanes, own_h)] = (gate / (1.0 + jnp.exp(-gate)) * upper).astype(jnp.bfloat16)
        turned = jnp.transpose(cw_ref[pl.ds(g * GROUP, GROUP)].reshape(GROUP * 2 * m, rows)).astype(jnp.bfloat16)
        for b in range(GROUP):
            code = jnp.dot(turned, ecode_ref[b], preferred_element_type=jnp.float32)
            value = jnp.dot(turned, ew_ref[b], preferred_element_type=jnp.float32)
            hit = (code + float(cap * b)) == place_ref[...]
            c_ref[g, pl.ds(b * rows, rows), pl.ds(0, lanes)] = jnp.where(hit, value, 0.0).astype(jnp.bfloat16)
    for q in range(1, m):
        gather_sd(q).wait_recv()
    for g in range(groups):
        for c in range(parts):
            rv_ref[g, c, pl.ds(lanes, own_h), :] = hd_ref[:, pl.ds(c * wide, wide)]

    def settle(w):
        for kind in range(3):
            weight_x_all(w, kind).wait_recv()
        for at in range(bundles[w][0], sum(bundles[w])):
            source = lax.rem(z + n + offset_of(order[at]), n)
            there = pl.ds(pl.multiple_of(source * deep, deep), deep)
            gate_ref[there, :] = jnp.transpose(fg_ref[:, pl.ds(at * deep, deep)])
            up_ref[there, :] = jnp.transpose(fu_ref[:, pl.ds(at * deep, deep)])
            down_ref[pl.ds(pl.multiple_of(source * down_rows, down_rows), down_rows), :] = fd_ref[
                pl.ds(at * down_rows, down_rows), :
            ]

    settled = 0
    for w in range(len(bundles)):
        if w not in moved_on:
            while settled < w - 1:
                settle(settled)
                settled += 1
            move_on(w)
    for w in range(settled, len(bundles)):
        settle(w)

    for g in range(groups):
        exchange_all(g).wait_send()
        exchange_all(g).wait_recv()

    def experts(first, count):
        @pl.loop(0, count)
        def _(i):
            g = first - i
            gate = jnp.zeros((lanes, gate_ref.shape[1]), jnp.float32)
            upper = jnp.zeros((lanes, gate_ref.shape[1]), jnp.float32)
            for c in range(parts):
                x = x_ref[g, c]
                deep_rows = pl.ds(c * wide, wide)
                gate += jnp.dot(x, gate_ref[deep_rows, :], preferred_element_type=jnp.float32)
                upper += jnp.dot(x, up_ref[deep_rows, :], preferred_element_type=jnp.float32)
            hidden = (gate / (1.0 + jnp.exp(-gate)) * upper).astype(jnp.bfloat16)

            @pl.loop(0, parts)
            def _(c):
                cols = pl.ds(pl.multiple_of(c * wide, wide), wide)
                y = jnp.dot(hidden, down_ref[:, cols], preferred_element_type=jnp.float32)
                stage_ref[g, c] = y.astype(jnp.bfloat16)
                rv_ref[g, c, of(tp), :] = stage_ref[g, c, of(tp), :]
                for q in range(1, m):
                    answer(g, c, q).start()

    def combine(g, c):
        answer_all(g, c).wait_recv()
        d_ref[c] = jnp.dot(c_ref[g], rv_ref[g, c], preferred_element_type=jnp.float32)

    def share(offset, c):
        return d_ref[c, pl.ds((slot_of(offset) % GROUP) * rows, rows), :]

    def hop(sign, r, c):
        if sign > 0:
            return remote(pst_ref.at[r % 2, c], pin_ref.at[r - 1, c],
                          p_send.at[r - 1, c], p_recv.at[r - 1, c], "fs", above)
        return remote(mst_ref.at[r % 2, c], min_ref.at[r - 1, c],
                      m_send.at[r - 1, c], m_recv.at[r - 1, c], "fs", below)

    def forward(sign, r, c):
        last = half - 1 if sign > 0 else half
        total = share(sign * r, c)
        if r < last:
            hop(sign, r + 1, c).wait_recv()
            total = total + (pin_ref if sign > 0 else min_ref)[r, c].astype(jnp.float32)
        if r + 2 <= last:
            hop(sign, r + 2, c).wait_send()
        (pst_ref if sign > 0 else mst_ref)[r % 2, c] = total.astype(jnp.bfloat16)
        hop(sign, r, c).start()

    early = min(2, groups)
    experts(groups - 1, early)
    for i in range(half):
        g = groups - 1 - i // 2

        @pl.loop(0, parts)
        def _(c):
            if i == 0:
                combine(g, c)
            forward(-1, half - i, c)
            if half - 1 - i > 0:
                forward(1, half - 1 - i, c)
            if i % 2 == 1 and g > 0:
                combine(g - 1, c)

        if i < groups - early:
            experts(groups - 1 - early - i, 1)

    @pl.loop(0, parts)
    def _(c):
        hop(1, 1, c).wait_recv()
        hop(-1, 1, c).wait_recv()
        total = share(0, c) + pin_ref[0, c].astype(jnp.float32) + min_ref[0, c].astype(jnp.float32)
        out_ref[:, pl.ds(pl.multiple_of(c * wide, wide), wide)] = total.astype(jnp.bfloat16)

    for c in range(parts):
        for r in range(1, min(2, half - 1) + 1):
            hop(1, r, c).wait_send()
        for r in range(1, min(2, half) + 1):
            hop(-1, r, c).wait_send()
        for g in range(groups):
            answer_all(g, c).wait_send()
    for q in range(1, m):
        gather_gu(q).wait_send()
        gather_sd(q).wait_send()
    for r in range(1, n):
        slice_gs(r).wait_send()
    for k in range(1, n):
        ring_meta(k).wait_send()
        for p in range(AG_PIECES):
            ring(k, p).wait_send()
    for w in range(len(bundles)):
        for kind in range(3):
            weight_z_all(w, kind).wait_send()
            weight_x_all(w, kind).wait_send()


def hand_on(
    mixed_ref, gate_ref, up_ref, down_ref, hgu_ref, hd_ref,
    mixed_out, gate_out, up_out, down_out, shared_gate_out, shared_up_out, shared_down_out,
):
    mixed_out[...] = mixed_ref[...]
    gate_out[0] = gate_ref[...]
    up_out[0] = up_ref[...]
    down_out[0] = down_ref[...]
    shared_gate_out[...] = jnp.transpose(hgu_ref[0])
    shared_up_out[...] = jnp.transpose(hgu_ref[1])
    shared_down_out[...] = hd_ref[...]


def on_device(
    tokens, route_ids, route_scores, norm_gain,
    expert_gate, expert_up, expert_down, shared_gate, shared_up, shared_down,
):
    n = lax.axis_size("fs")
    m = lax.axis_size("tp")
    experts = n * m
    rows, width = tokens.shape
    picks = route_ids.shape[1]
    cap = 3 * rows * picks // (2 * experts)
    slots = GROUP * cap
    lanes = m * slots
    groups = n // GROUP
    half = n // 2
    bf16, f32 = jnp.bfloat16, jnp.float32
    dma = pltpu.SemaphoreType.DMA
    wide = min(512, width)
    parts = width // wide

    deep, cols_f = expert_gate.shape[1:]
    down_rows, down_cols = expert_down.shape[1:]
    hidden = m * cols_f
    own_h = hidden // n

    def turned(weight):
        return jnp.swapaxes(weight, 1, 2).reshape(n, m, cols_f, deep)

    lane = np.arange(lanes)
    row = np.arange(GROUP * 2 * m)
    block = np.arange(GROUP)

    def expand(first):
        wanted = block[:, None, None] * 2 * m + first + (lane // slots)[None, None, :]
        return jnp.asarray((row[None, :, None] == wanted).astype(np.float32), bf16)

    place = jnp.asarray((lane % slots)[None, :].astype(np.float32))
    held = pl.BlockSpec(memory_space=pl.ANY)
    results = pl.pallas_call(
        functools.partial(kernel, n, m, cap),
        out_shape=(
            jax.ShapeDtypeStruct((rows, width), bf16),
            jax.ShapeDtypeStruct((width, hidden), bf16),
            jax.ShapeDtypeStruct((width, hidden), bf16),
            jax.ShapeDtypeStruct((hidden, width), bf16),
            jax.ShapeDtypeStruct((2, hidden, deep), bf16),
            jax.ShapeDtypeStruct((down_rows, width), bf16),
        ),
        in_specs=[VMEM] * 7 + [held] * 3 + [VMEM] * 3,
        out_specs=(VMEM,) * 6,
        scratch_shapes=[
            pltpu.VMEM((n * rows, width), bf16),
            pltpu.VMEM((n, 2 * picks, rows), f32),
            pltpu.VMEM((n, 2 * m, rows), f32),
            pltpu.VMEM((groups, parts, lanes, wide), bf16),
            pltpu.VMEM((groups, parts, lanes, wide), bf16),
            pltpu.VMEM((groups, parts, lanes + own_h, wide), bf16),
            pltpu.VMEM((lanes, GROUP * rows), bf16),
            pltpu.VMEM((2, own_h, width), bf16),
            pltpu.VMEM((2, cols_f, deep), bf16),
            pltpu.VMEM((down_rows, down_cols), bf16),
            pltpu.VMEM((2, n // LOADS, m, cols_f, deep), f32),
            pltpu.VMEM((2, n // LOADS, m, cols_f, deep), f32),
            pltpu.VMEM((2, n // LOADS, m, down_rows, down_cols), f32),
            pltpu.VMEM((n, m, cols_f, deep), bf16),
            pltpu.VMEM((n, m, cols_f, deep), bf16),
            pltpu.VMEM((n, m, down_rows, down_cols), bf16),
            pltpu.VMEM((m, cols_f, width), bf16),
            pltpu.VMEM((m, cols_f, width), bf16),
            pltpu.VMEM((m, n * down_rows, down_cols), bf16),
            pltpu.VMEM((hidden, width), bf16),
            pltpu.VMEM((hidden, width), bf16),
            pltpu.VMEM((hidden, width), bf16),
            pltpu.VMEM((groups, GROUP * rows, lanes + own_h), bf16),
            pltpu.VMEM((parts, GROUP * rows, wide), f32),
            pltpu.VMEM((half, parts, rows, wide), bf16),
            pltpu.VMEM((half, parts, rows, wide), bf16),
            pltpu.VMEM((2, parts, rows, wide), bf16),
            pltpu.VMEM((2, parts, rows, wide), bf16),
            dma((n, AG_PIECES)), dma((n, AG_PIECES)), dma((n,)), dma((n,)),
            dma((groups,)), dma((groups,)), dma((groups, parts)), dma((groups, parts)),
            dma((m - 1,)), dma((m - 1,)), dma((m - 1,)), dma((m - 1,)), dma((n - 1,)), dma((n - 1,)),
            dma((2, 3)), *[dma((groups + 1, 3))] * 4,
            *[dma((half, parts))] * 4,
        ],
        compiler_params=pltpu.CompilerParams(
            collective_id=0, has_side_effects=True, vmem_limit_bytes=63 * 1024 * 1024,
        ),
        cost_estimate=pl.CostEstimate(flops=100_000_000_000, bytes_accessed=30_000_000, transcendentals=0),
        name="hand_over",
    )(
        tokens, route_ids.T, route_scores.T, norm_gain[None, :], shared_gate.T, shared_up.T, shared_down,
        turned(expert_gate), turned(expert_up), expert_down.reshape(n, m, down_rows, down_cols),
        expand(0), expand(m), place,
    )
    whole = jax.ShapeDtypeStruct((1, width, hidden), bf16)
    held_up = jax.ShapeDtypeStruct((deep, hidden), bf16)
    return pl.pallas_call(
        hand_on,
        out_shape=(
            jax.ShapeDtypeStruct((rows, width), bf16), whole, whole, jax.ShapeDtypeStruct((1, hidden, width), bf16),
            held_up, held_up, jax.ShapeDtypeStruct((down_rows, width), bf16),
        ),
        in_specs=[VMEM] * 6,
        out_specs=(VMEM,) * 7,
        cost_estimate=pl.CostEstimate(flops=1_000_000, bytes_accessed=8_000_000, transcendentals=0),
        name="hand_on",
    )(*results)


def solution(mesh):
    return jax.shard_map(
        on_device,
        mesh=mesh,
        in_specs=(
            P(("grp", "fs", "tp"), None),
            P(("grp", "fs", "tp"), None),
            P(("grp", "fs", "tp"), None),
            P("fs"),
            P(None, "fs", "tp"),
            P(None, "fs", "tp"),
            P(None, "fs", "tp"),
            P("fs", "tp"),
            P("fs", "tp"),
            P("fs", "tp"),
        ),
        out_specs=(
            P(("grp", "fs", "tp"), None),
            P(("grp", "fs", "tp"), None, None),
            P(("grp", "fs", "tp"), None, None),
            P(("grp", "fs", "tp"), None, None),
            P(("grp", "fs"), None),
            P(("grp", "fs"), None),
            P(("grp", "fs"), None),
        ),
        check_vma=False,
    )
```

```python
import functools

import jax
import jax.numpy as jnp
import numpy as np
from jax import lax
from jax.experimental import pallas as pl
from jax.experimental.pallas import tpu as pltpu
from jax.sharding import PartitionSpec as P

EPSILON = 1e-06
route_scale = 2.5
ABSENT = -1024.0
MESH = pl.DeviceIdType.MESH
GROUP = 4
AG_PIECES = 2
LOADS = 4
VMEM = pl.BlockSpec(memory_space=pltpu.VMEM)


def slot_of(offset):
    return 2 * offset if offset >= 0 else -2 * offset - 1


def greet(names_and_counts):
    barrier = pltpu.get_barrier_semaphore()
    total = 0
    for name, steps in names_and_counts:
        size = lax.axis_size(name)
        me = lax.axis_index(name)
        for step in steps:
            peer = lax.rem(me + step + size, size)
            pl.semaphore_signal(barrier, inc=1, device_id={name: peer}, device_id_type=MESH)
            total += 1
    return barrier, total


def remote(src, dst, send, recv, name, peer):
    return pltpu.make_async_remote_copy(
        src_ref=src, dst_ref=dst, send_sem=send, recv_sem=recv,
        device_id={name: peer}, device_id_type=MESH,
    )


def offset_of(slot):
    return slot // 2 if slot % 2 == 0 else -((slot + 1) // 2)


def weight_order(n):
    order, far, near = [0, n - 1], n - 2, 1
    while near < far:
        order += [far, far - 1]
        far -= 2
        if near < far:
            order += [near, near + 1]
            near += 2
    return order


def kernel(
    n, m, cap, tok_ref, ids_ref, sc_ref, gain_ref, sg_ref, su_ref, sd32_ref, eg_ref, eu_ref, ed_ref,
    ecode_ref, ew_ref, place_ref,
    out_ref, gate_ref, up_ref, down_ref, hgu_ref, hd_ref,
    all_ref, meta_ref, cw_ref, stage_ref, x_ref, rv_ref, pick_ref, gs_ref,
    sgu_ref, sd_ref, eg32_ref, eu32_ref, ed32_ref, wg_ref, wu_ref, wd_ref,
    mg_ref, mu_ref, md_ref, fg_ref, fu_ref, fd_ref, c_ref, d_ref, pin_ref, min_ref, pst_ref, mst_ref,
    ag_send, ag_recv, meta_send, meta_recv, x_send, x_recv, y_send, y_recv,
    gu_send, gu_recv, sd_send, sd_recv, gs_send, gs_recv,
    load_sem, wz_send, wz_recv, wx_send, wx_recv, p_send, p_recv, m_send, m_recv,
):
    z, tp = lax.axis_index("fs"), lax.axis_index("tp")
    rows, width = tok_ref.shape
    picks = ids_ref.shape[0]
    above, below = lax.rem(z + 1, n), lax.rem(z + n - 1, n)
    parts, wide = stage_ref.shape[1], stage_ref.shape[3]
    slots = GROUP * cap
    lanes = m * slots
    half, groups = n // 2, n // GROUP
    cols_f, deep = sgu_ref.shape[1:]
    order = weight_order(n)
    bundles = [(first, GROUP) for first in range(0, n - GROUP, GROUP)] + [(n - GROUP, GROUP - 1), (n - 1, 1)]
    bundle_of = [w for w, (_, count) in enumerate(bundles) for _ in range(count)]
    own_h = gs_ref.shape[1]
    down_rows, down_cols = sd_ref.shape

    def tp_rows(size):
        return pl.ds(pl.multiple_of(tp * size, size), size)

    barrier, arrivals = greet((("fs", range(1, n)), ("tp", range(1, m))))
    widened = tok_ref[...].astype(jnp.float32)
    scale = lax.rsqrt(jnp.mean(widened * widened, axis=1, keepdims=True) + EPSILON)
    all_ref[pl.ds(0, rows), :] = (widened * scale).astype(jnp.bfloat16)
    scores = sc_ref[...]
    meta_ref[0, pl.ds(0, picks), :] = ids_ref[...].astype(jnp.float32)
    meta_ref[0, pl.ds(picks, picks), :] = route_scale * scores / jnp.sum(scores, axis=0, keepdims=True)
    gain = gain_ref[...]
    sgu_ref[0] = (gain * sg_ref[...]).astype(jnp.bfloat16)
    sgu_ref[1] = (gain * su_ref[...]).astype(jnp.bfloat16)
    sd_ref[...] = sd32_ref[...].astype(jnp.bfloat16)
    hgu_ref[:, tp_rows(cols_f), :] = sgu_ref[...]
    hd_ref[:, tp_rows(down_cols)] = sd_ref[...]
    pl.semaphore_wait(barrier, arrivals)

    step_rows = rows // AG_PIECES

    def ring(k, p):
        src = max(k - 2, 0)
        return remote(
            all_ref.at[pl.ds(src * rows + p * step_rows, step_rows), :],
            all_ref.at[pl.ds(k * rows + p * step_rows, step_rows), :],
            ag_send.at[k, p], ag_recv.at[k, p], "fs", above if k % 2 == 1 else below,
        )

    def ring_meta(k):
        return remote(
            meta_ref.at[max(k - 2, 0)], meta_ref.at[k], meta_send.at[k], meta_recv.at[k],
            "fs", above if k % 2 == 1 else below,
        )

    def gather_gu(q):
        return remote(
            sgu_ref, hgu_ref.at[:, tp_rows(cols_f), :], gu_send.at[q - 1], gu_recv.at[q - 1], "tp", lax.rem(tp + q, m)
        )

    def gather_sd(q):
        return remote(
            sd_ref, hd_ref.at[:, tp_rows(down_cols)], sd_send.at[q - 1], sd_recv.at[q - 1], "tp", lax.rem(tp + q, m)
        )

    def slice_gs(r):
        peer = lax.rem(z + r, n)
        return remote(
            hgu_ref.at[:, pl.ds(pl.multiple_of(peer * own_h, own_h), own_h), :],
            gs_ref.at[:, :, pl.ds(pl.multiple_of(z * deep, deep), deep)],
            gs_send.at[r - 1], gs_recv.at[r - 1], "fs", peer,
        )

    kinds = (
        (wg_ref, mg_ref, fg_ref), (wu_ref, mu_ref, fu_ref), (wd_ref, md_ref, fd_ref),
    )

    def mid_place(kind, first, count):
        if kind < 2:
            return (slice(None), slice(None), pl.ds(first * deep, count * deep))
        return (slice(None), pl.ds(first * down_rows, count * down_rows), slice(None))

    def weight_z(at, kind):
        peer = lax.rem(z + n - offset_of(order[at]), n)
        src, mid, _ = kinds[kind]
        w = bundle_of[at]
        return remote(
            src.at[peer], mid.at[mid_place(kind, at, 1)], wz_send.at[w, kind], wz_recv.at[w, kind], "fs", peer
        )

    def weight_z_all(w, kind):
        first, count = bundles[w]
        first, count = max(1, first), count - (first == 0)
        _, mid, _ = kinds[kind]
        return remote(
            mid.at[mid_place(kind, first, count)], mid.at[mid_place(kind, first, count)],
            wz_send.at[w, kind], wz_recv.at[w, kind], "fs", above,
        )

    def piece(w, kind, who):
        first, count = bundles[w]
        if kind < 2:
            return who, slice(None), pl.ds(first * deep, count * deep)
        return who, pl.ds(first * down_rows, count * down_rows), slice(None)

    def landing(w, kind, where):
        first, count = bundles[w]
        if kind < 2:
            return where, pl.ds(first * deep, count * deep)
        return pl.ds(first * down_rows, count * down_rows), where

    def weight_x(w, q, kind):
        peer = lax.rem(tp + q, m)
        _, mid, final = kinds[kind]
        where = tp_rows(cols_f if kind < 2 else down_cols)
        return remote(
            mid.at[piece(w, kind, peer)], final.at[landing(w, kind, where)],
            wx_send.at[w, kind], wx_recv.at[w, kind], "tp", peer,
        )

    def weight_x_all(w, kind):
        _, _, final = kinds[kind]
        where = pl.ds(0, (m - 1) * (cols_f if kind < 2 else down_cols))
        return remote(
            final.at[landing(w, kind, where)], final.at[landing(w, kind, where)],
            wx_send.at[w, kind], wx_recv.at[w, kind], "tp", lax.rem(tp + 1, m),
        )

    def of(who):
        return pl.ds(pl.multiple_of(who * slots, slots), slots)

    most = pl.ds(0, (m - 1) * slots)

    def exchange(g, q):
        peer = lax.rem(tp + q, m)
        return remote(stage_ref.at[g, :, of(peer)], x_ref.at[g, :, of(tp)], x_send.at[g], x_recv.at[g], "tp", peer)

    def exchange_all(g):
        return remote(
            stage_ref.at[g, :, most], x_ref.at[g, :, most], x_send.at[g], x_recv.at[g], "tp", lax.rem(tp + 1, m)
        )

    def answer(g, c, q):
        peer = lax.rem(tp + q, m)
        return remote(
            stage_ref.at[g, c, of(peer)], rv_ref.at[g, c, of(tp)], y_send.at[g, c], y_recv.at[g, c], "tp", peer
        )

    def answer_all(g, c):
        return remote(
            stage_ref.at[g, c, most], rv_ref.at[g, c, most], y_send.at[g, c], y_recv.at[g, c], "tp", lax.rem(tp + 1, m)
        )

    span = n // LOADS
    loads = ((eg_ref, eg32_ref), (eu_ref, eu32_ref), (ed_ref, ed32_ref))

    def load(i, kind):
        src, dst = loads[kind]
        return pltpu.make_async_copy(src.at[pl.ds(i * span, span)], dst.at[i % 2], load_sem.at[i % 2, kind])

    for kind in range(3):
        load(0, kind).start()
    for k in (1, 2):
        ring_meta(k).start()
        for p in range(AG_PIECES):
            ring(k, p).start()
    for q in range(1, m):
        gather_gu(q).start()
        gather_sd(q).start()
    for i in range(LOADS):
        for kind in range(3):
            if i + 1 < LOADS:
                load(i + 1, kind).start()
            load(i, kind).wait()
        some = pl.ds(i * span, span)
        wg_ref[some] = (gain * eg32_ref[i % 2]).astype(jnp.bfloat16)
        wu_ref[some] = (gain * eu32_ref[i % 2]).astype(jnp.bfloat16)
        wd_ref[some] = ed32_ref[i % 2].astype(jnp.bfloat16)
    for kind, (src, mid, _) in enumerate(kinds):
        mid[mid_place(kind, 0, 1)] = src[z]
    for q in range(1, m):
        gather_gu(q).wait_recv()
    for r in range(1, n):
        slice_gs(r).start()
    gs_ref[:, :, pl.ds(pl.multiple_of(z * deep, deep), deep)] = hgu_ref[
        :, pl.ds(pl.multiple_of(z * own_h, own_h), own_h), :
    ]

    before = lax.broadcasted_iota(jnp.int32, (rows, rows), 0) < lax.broadcasted_iota(jnp.int32, (rows, rows), 1)
    before = before.astype(jnp.float32).astype(jnp.bfloat16)
    served = (lax.broadcasted_iota(jnp.int32, (m, rows), 0) + m * z).astype(jnp.float32)
    places = lax.broadcasted_iota(jnp.int32, (slots, rows), 0).astype(jnp.float32)

    def select(g):
        for b in range(GROUP):
            k = g * GROUP + b
            meta = meta_ref[k]
            chosen = jnp.zeros((m, rows), jnp.float32)
            weight = jnp.zeros((m, rows), jnp.float32)
            for j in range(picks):
                hit = meta[j : j + 1, :] == served
                chosen = chosen + hit.astype(jnp.float32)
                weight = weight + jnp.where(hit, meta[picks + j : picks + j + 1, :], 0.0)
            rank = jnp.dot(chosen.astype(jnp.bfloat16), before, preferred_element_type=jnp.float32)
            code = jnp.where(chosen > 0.0, rank, ABSENT)
            cw_ref[k, pl.ds(0, m), :] = code
            cw_ref[k, pl.ds(m, m), :] = weight
            for q in range(m):
                hot = (jnp.broadcast_to(code[q : q + 1, :], (slots, rows)) + float(cap * b)) == places
                pick_ref[pl.ds(q * slots, slots), pl.ds(b * rows, rows)] = hot.astype(jnp.float32).astype(jnp.bfloat16)

        @pl.loop(0, parts)
        def _(c):
            cols = pl.ds(pl.multiple_of(c * wide, wide), wide)
            taken = jnp.dot(
                pick_ref[...], all_ref[pl.ds(g * GROUP * rows, GROUP * rows), cols],
                preferred_element_type=jnp.float32,
            ).astype(jnp.bfloat16)
            stage_ref[g, c] = taken
            x_ref[g, c, of(tp), :] = stage_ref[g, c, of(tp), :]

        for q in range(1, m):
            exchange(g, q).start()

    moved_on = []

    def move_on(w):
        moved_on.append(w)
        for kind in range(3):
            weight_z_all(w, kind).wait_recv()
        for q in range(1, m):
            for kind in range(3):
                weight_x(w, q, kind).start()
        for kind, (_, mid, final) in enumerate(kinds):
            where = tp_rows(cols_f if kind < 2 else down_cols)
            final[landing(w, kind, where)] = mid[piece(w, kind, tp)]

    issue = {}
    for at in range(1, n):
        issue.setdefault(max(1, min(n - 3, 1 + 2 * (at // 2))), []).append(at)
    for k in range(1, n):
        ring_meta(k).wait_recv()
        if k + 2 < n:
            ring_meta(k + 2).start()
        for p in range(AG_PIECES):
            ring(k, p).wait_recv()
            if k + 2 < n:
                ring(k + 2, p).start()
        for at in issue.get(k, ()):
            for kind in range(3):
                weight_z(at, kind).start()
        if k % GROUP == GROUP - 1:
            select(k // GROUP)
            if groups > 2 and k // GROUP >= groups - 2:
                move_on(k // GROUP - groups + 2)

    for r in range(1, n):
        slice_gs(r).wait_recv()
    for g in range(groups):
        some = pl.ds(g * GROUP * rows, GROUP * rows)
        both = lax.dot_general(
            all_ref[some, :], gs_ref[...].reshape(2 * own_h, width), (((1,), (1,)), ((), ())),
            preferred_element_type=jnp.float32,
        )
        gate, upper = both[:, :own_h], both[:, own_h:]
        c_ref[g, :, pl.ds(lanes, own_h)] = (gate / (1.0 + jnp.exp(-gate)) * upper).astype(jnp.bfloat16)
        turned = jnp.transpose(cw_ref[pl.ds(g * GROUP, GROUP)].reshape(GROUP * 2 * m, rows)).astype(jnp.bfloat16)
        for b in range(GROUP):
            code = jnp.dot(turned, ecode_ref[b], preferred_element_type=jnp.float32)
            value = jnp.dot(turned, ew_ref[b], preferred_element_type=jnp.float32)
            hit = (code + float(cap * b)) == place_ref[...]
            c_ref[g, pl.ds(b * rows, rows), pl.ds(0, lanes)] = jnp.where(hit, value, 0.0).astype(jnp.bfloat16)
    for q in range(1, m):
        gather_sd(q).wait_recv()
    for g in range(groups):
        for c in range(parts):
            rv_ref[g, c, pl.ds(lanes, own_h), :] = hd_ref[:, pl.ds(c * wide, wide)]

    def settle(w):
        for kind in range(3):
            weight_x_all(w, kind).wait_recv()
        for at in range(bundles[w][0], sum(bundles[w])):
            source = lax.rem(z + n + offset_of(order[at]), n)
            there = pl.ds(pl.multiple_of(source * deep, deep), deep)
            gate_ref[there, :] = jnp.transpose(fg_ref[:, pl.ds(at * deep, deep)])
            up_ref[there, :] = jnp.transpose(fu_ref[:, pl.ds(at * deep, deep)])
            down_ref[pl.ds(pl.multiple_of(source * down_rows, down_rows), down_rows), :] = fd_ref[
                pl.ds(at * down_rows, down_rows), :
            ]

    settled = 0
    for w in range(len(bundles)):
        if w not in moved_on:
            while settled < w - 1:
                settle(settled)
                settled += 1
            move_on(w)
    for w in range(settled, len(bundles)):
        settle(w)

    for g in range(groups):
        exchange_all(g).wait_send()
        exchange_all(g).wait_recv()

    def experts(first, count):
        @pl.loop(0, count)
        def _(i):
            g = first - i
            gate = jnp.zeros((lanes, gate_ref.shape[1]), jnp.float32)
            upper = jnp.zeros((lanes, gate_ref.shape[1]), jnp.float32)
            for c in range(parts):
                x = x_ref[g, c]
                deep_rows = pl.ds(c * wide, wide)
                gate += jnp.dot(x, gate_ref[deep_rows, :], preferred_element_type=jnp.float32)
                upper += jnp.dot(x, up_ref[deep_rows, :], preferred_element_type=jnp.float32)
            hidden = (gate / (1.0 + jnp.exp(-gate)) * upper).astype(jnp.bfloat16)

            @pl.loop(0, parts)
            def _(c):
                cols = pl.ds(pl.multiple_of(c * wide, wide), wide)
                y = jnp.dot(hidden, down_ref[:, cols], preferred_element_type=jnp.float32)
                stage_ref[g, c] = y.astype(jnp.bfloat16)
                rv_ref[g, c, of(tp), :] = stage_ref[g, c, of(tp), :]
                for q in range(1, m):
                    answer(g, c, q).start()

    def combine(g, c):
        answer_all(g, c).wait_recv()
        d_ref[c] = jnp.dot(c_ref[g], rv_ref[g, c], preferred_element_type=jnp.float32)

    def share(offset, c):
        return d_ref[c, pl.ds((slot_of(offset) % GROUP) * rows, rows), :]

    def hop(sign, r, c):
        if sign > 0:
            return remote(pst_ref.at[r % 2, c], pin_ref.at[r - 1, c],
                          p_send.at[r - 1, c], p_recv.at[r - 1, c], "fs", above)
        return remote(mst_ref.at[r % 2, c], min_ref.at[r - 1, c],
                      m_send.at[r - 1, c], m_recv.at[r - 1, c], "fs", below)

    def forward(sign, r, c):
        last = half - 1 if sign > 0 else half
        total = share(sign * r, c)
        if r < last:
            hop(sign, r + 1, c).wait_recv()
            total = total + (pin_ref if sign > 0 else min_ref)[r, c].astype(jnp.float32)
        if r + 2 <= last:
            hop(sign, r + 2, c).wait_send()
        (pst_ref if sign > 0 else mst_ref)[r % 2, c] = total.astype(jnp.bfloat16)
        hop(sign, r, c).start()

    early = min(2, groups)
    experts(groups - 1, early)
    for i in range(half):
        g = groups - 1 - i // 2

        @pl.loop(0, parts)
        def _(c):
            if i == 0:
                combine(g, c)
            forward(-1, half - i, c)
            if half - 1 - i > 0:
                forward(1, half - 1 - i, c)
            if i % 2 == 1 and g > 0:
                combine(g - 1, c)

        if i < groups - early:
            experts(groups - 1 - early - i, 1)

    @pl.loop(0, parts)
    def _(c):
        hop(1, 1, c).wait_recv()
        hop(-1, 1, c).wait_recv()
        total = share(0, c) + pin_ref[0, c].astype(jnp.float32) + min_ref[0, c].astype(jnp.float32)
        out_ref[:, pl.ds(pl.multiple_of(c * wide, wide), wide)] = total.astype(jnp.bfloat16)

    for c in range(parts):
        for r in range(1, min(2, half - 1) + 1):
            hop(1, r, c).wait_send()
        for r in range(1, min(2, half) + 1):
            hop(-1, r, c).wait_send()
        for g in range(groups):
            answer_all(g, c).wait_send()
    for q in range(1, m):
        gather_gu(q).wait_send()
        gather_sd(q).wait_send()
    for r in range(1, n):
        slice_gs(r).wait_send()
    for k in range(1, n):
        ring_meta(k).wait_send()
        for p in range(AG_PIECES):
            ring(k, p).wait_send()
    for w in range(len(bundles)):
        for kind in range(3):
            weight_z_all(w, kind).wait_send()
            weight_x_all(w, kind).wait_send()


def hand_on(
    mixed_ref, gate_ref, up_ref, down_ref, hgu_ref, hd_ref,
    mixed_out, gate_out, up_out, down_out, shared_gate_out, shared_up_out, shared_down_out,
):
    mixed_out[...] = mixed_ref[...]
    gate_out[0] = gate_ref[...]
    up_out[0] = up_ref[...]
    down_out[0] = down_ref[...]
    shared_gate_out[...] = jnp.transpose(hgu_ref[0])
    shared_up_out[...] = jnp.transpose(hgu_ref[1])
    shared_down_out[...] = hd_ref[...]


def on_device(
    tokens, route_ids, route_scores, norm_gain,
    expert_gate, expert_up, expert_down, shared_gate, shared_up, shared_down,
):
    n = lax.axis_size("fs")
    m = lax.axis_size("tp")
    experts = n * m
    rows, width = tokens.shape
    picks = route_ids.shape[1]
    cap = 3 * rows * picks // (2 * experts)
    slots = GROUP * cap
    lanes = m * slots
    groups = n // GROUP
    half = n // 2
    bf16, f32 = jnp.bfloat16, jnp.float32
    dma = pltpu.SemaphoreType.DMA
    wide = min(512, width)
    parts = width // wide

    deep, cols_f = expert_gate.shape[1:]
    down_rows, down_cols = expert_down.shape[1:]
    hidden = m * cols_f
    own_h = hidden // n

    def turned(weight):
        return jnp.swapaxes(weight, 1, 2).reshape(n, m, cols_f, deep)

    lane = np.arange(lanes)
    row = np.arange(GROUP * 2 * m)
    block = np.arange(GROUP)

    def expand(first):
        wanted = block[:, None, None] * 2 * m + first + (lane // slots)[None, None, :]
        return jnp.asarray((row[None, :, None] == wanted).astype(np.float32), bf16)

    place = jnp.asarray((lane % slots)[None, :].astype(np.float32))
    held = pl.BlockSpec(memory_space=pl.ANY)
    results = pl.pallas_call(
        functools.partial(kernel, n, m, cap),
        out_shape=(
            jax.ShapeDtypeStruct((rows, width), bf16),
            jax.ShapeDtypeStruct((width, hidden), bf16),
            jax.ShapeDtypeStruct((width, hidden), bf16),
            jax.ShapeDtypeStruct((hidden, width), bf16),
            jax.ShapeDtypeStruct((2, hidden, deep), bf16),
            jax.ShapeDtypeStruct((down_rows, width), bf16),
        ),
        in_specs=[VMEM] * 7 + [held] * 3 + [VMEM] * 3,
        out_specs=(VMEM,) * 6,
        scratch_shapes=[
            pltpu.VMEM((n * rows, width), bf16),
            pltpu.VMEM((n, 2 * picks, rows), f32),
            pltpu.VMEM((n, 2 * m, rows), f32),
            pltpu.VMEM((groups, parts, lanes, wide), bf16),
            pltpu.VMEM((groups, parts, lanes, wide), bf16),
            pltpu.VMEM((groups, parts, lanes + own_h, wide), bf16),
            pltpu.VMEM((lanes, GROUP * rows), bf16),
            pltpu.VMEM((2, own_h, width), bf16),
            pltpu.VMEM((2, cols_f, deep), bf16),
            pltpu.VMEM((down_rows, down_cols), bf16),
            pltpu.VMEM((2, n // LOADS, m, cols_f, deep), f32),
            pltpu.VMEM((2, n // LOADS, m, cols_f, deep), f32),
            pltpu.VMEM((2, n // LOADS, m, down_rows, down_cols), f32),
            pltpu.VMEM((n, m, cols_f, deep), bf16),
            pltpu.VMEM((n, m, cols_f, deep), bf16),
            pltpu.VMEM((n, m, down_rows, down_cols), bf16),
            pltpu.VMEM((m, cols_f, width), bf16),
            pltpu.VMEM((m, cols_f, width), bf16),
            pltpu.VMEM((m, n * down_rows, down_cols), bf16),
            pltpu.VMEM((hidden, width), bf16),
            pltpu.VMEM((hidden, width), bf16),
            pltpu.VMEM((hidden, width), bf16),
            pltpu.VMEM((groups, GROUP * rows, lanes + own_h), bf16),
            pltpu.VMEM((parts, GROUP * rows, wide), f32),
            pltpu.VMEM((half, parts, rows, wide), bf16),
            pltpu.VMEM((half, parts, rows, wide), bf16),
            pltpu.VMEM((2, parts, rows, wide), bf16),
            pltpu.VMEM((2, parts, rows, wide), bf16),
            dma((n, AG_PIECES)), dma((n, AG_PIECES)), dma((n,)), dma((n,)),
            dma((groups,)), dma((groups,)), dma((groups, parts)), dma((groups, parts)),
            dma((m - 1,)), dma((m - 1,)), dma((m - 1,)), dma((m - 1,)), dma((n - 1,)), dma((n - 1,)),
            dma((2, 3)), *[dma((groups + 1, 3))] * 4,
            *[dma((half, parts))] * 4,
        ],
        compiler_params=pltpu.CompilerParams(
            collective_id=0, has_side_effects=True, vmem_limit_bytes=63 * 1024 * 1024,
        ),
        cost_estimate=pl.CostEstimate(flops=100_000_000_000, bytes_accessed=30_000_000, transcendentals=0),
        name="hand_over",
    )(
        tokens, route_ids.T, route_scores.T, norm_gain[None, :], shared_gate.T, shared_up.T, shared_down,
        turned(expert_gate), turned(expert_up), expert_down.reshape(n, m, down_rows, down_cols),
        expand(0), expand(m), place,
    )
    whole = jax.ShapeDtypeStruct((1, width, hidden), bf16)
    held_up = jax.ShapeDtypeStruct((deep, hidden), bf16)
    return pl.pallas_call(
        hand_on,
        out_shape=(
            jax.ShapeDtypeStruct((rows, width), bf16), whole, whole, jax.ShapeDtypeStruct((1, hidden, width), bf16),
            held_up, held_up, jax.ShapeDtypeStruct((down_rows, width), bf16),
        ),
        in_specs=[VMEM] * 6,
        out_specs=(VMEM,) * 7,
        cost_estimate=pl.CostEstimate(flops=1_000_000, bytes_accessed=8_000_000, transcendentals=0),
        name="hand_on",
    )(*results)


def solution(mesh):
    return jax.shard_map(
        on_device,
        mesh=mesh,
        in_specs=(
            P(("grp", "fs", "tp"), None),
            P(("grp", "fs", "tp"), None),
            P(("grp", "fs", "tp"), None),
            P("fs"),
            P(None, "fs", "tp"),
            P(None, "fs", "tp"),
            P(None, "fs", "tp"),
            P("fs", "tp"),
            P("fs", "tp"),
            P("fs", "tp"),
        ),
        out_specs=(
            P(("grp", "fs", "tp"), None),
            P(("grp", "fs", "tp"), None, None),
            P(("grp", "fs", "tp"), None, None),
            P(("grp", "fs", "tp"), None, None),
            P(("grp", "fs"), None),
            P(("grp", "fs"), None),
            P(("grp", "fs"), None),
        ),
        check_vma=False,
    )
```
